512 devices in a mesh: tp: 64 (over z, y), dp: 8 (over x, core).
Axes of the slice: x: 4, y: 4, z: 16, core: 2. Of those that a mesh axis runs over, the one named last changes fastest.
Arguments:
- resid: bfloat16 [256, 2048], P('dp', 'tp'), may hold values from -6 to 6
- norm_gain: float32 [2, 2048], replicated, may hold values from 0.1 to 1.9
- w_query: bfloat16 [2, 2048, 2048], P(None, 'dp', 'tp'), may hold values from -0.125 to 0.125
- w_forget: bfloat16 [2, 2048, 2048], P(None, 'dp', 'tp'), may hold values from -0.125 to 0.125
- w_value: bfloat16 [2, 2048, 16, 128], P(None, 'dp', None, 'tp'), may hold values from -0.125 to 0.125
- w_gate: bfloat16 [2, 2048, 16, 128], P(None, 'dp', None, 'tp'), may hold values from -0.125 to 0.125
- gate_floor: float32 [2, 2048], replicated, may hold values from 0 to 0.9
- states: float32 [2, 256, 16, 128, 128], P(None, 'dp', None, 'tp'), may hold values from -1 to 1
- out_gain: float32 [2, 16, 128], P(None, None, 'tp'), may hold values from 0.1 to 1.9
- w_out: bfloat16 [2, 16, 128, 2048], P(None, None, 'tp'), may hold values from -0.125 to 0.125
Outputs:
- new_resid: bfloat16 [256, 2048], P('dp', 'tp')
- new_states: float32 [2, 256, 16, 128, 128], P(None, 'dp', None, 'tp')
The draws below stay inside these ranges and needn't reach their ends.
All inputs are finite; a program needn't handle non-finite values.
Results may differ from the reference program's by a relative error of at most 0.029.
Values may be sent and summed in bfloat16 or wider, within the bound.
A program may use at most 64 MiB of HBM per device.

```python
import jax
import jax.numpy as jnp
from jax import lax

D = 2048
HEADS = 16
HD = 128
BLOCKS = 2
WIDTH = 2048
BATCH = 256
N_DP = 8


def block_scale(own_key, dims, split, low, largest):
    def one(axis_at, shards_of):
        heights = jax.random.uniform(jax.random.fold_in(jax.random.fold_in(own_key, 6), axis_at), (shards_of,), jnp.float32, low / len(split), largest / len(split))
        return jnp.repeat(jnp.exp(heights), dims[axis_at] // shards_of).reshape((-1,) + (1,) * (len(dims) - axis_at - 1))

    gain = one(*split[0])
    for cut in split[1:]:
        gain = gain * one(*cut)
    return gain


def normal_values(key, extent, deviation, bound, cuts=(), kind=jnp.bfloat16):
    values = jax.random.normal(key, extent, jnp.float32) * deviation
    if len(cuts) > 0:
        values = block_scale(key, extent, cuts, -0.22, 0.18) * values
    return jnp.clip(values, min=-bound, max=bound).astype(kind)


def setup_inputs(seed: int = 0) -> dict:
    key_of = jax.random.split(jax.random.key(seed), 11)
    return {
        "resid": normal_values(key_of[0], (BATCH, D), 1.0, 6.0, ((0, 8), (1, 64))),
        "norm_gain": jnp.clip(1.0 + 0.18 * jax.random.normal(key_of[1], (BLOCKS, D), jnp.float32), 0.1, 1.9),
        "w_query": normal_values(key_of[2], (BLOCKS, D, WIDTH), D ** -0.5, 0.125, ((1, 8), (2, 64))),
        "w_forget": normal_values(key_of[3], (BLOCKS, D, WIDTH), D ** -0.5, 0.125, ((1, 8), (2, 64))),
        "w_value": normal_values(key_of[4], (BLOCKS, D, HEADS, HD), D ** -0.5, 0.125, ((1, 8), (3, 64))),
        "w_gate": normal_values(key_of[5], (BLOCKS, D, HEADS, HD), D ** -0.5, 0.125, ((1, 8), (3, 64))),
        "gate_floor": jnp.clip(jax.random.uniform(key_of[6], (BLOCKS, WIDTH), jnp.float32, 0.0, 0.9), 0.0, 0.9),
        "states": normal_values(key_of[7], (BLOCKS, BATCH, HEADS, HD, HD), 0.15, 1.0, ((1, 8), (3, 64)), jnp.float32),
        "out_gain": jnp.clip(1.0 + 0.18 * jax.random.normal(key_of[8], (BLOCKS, HEADS, HD), jnp.float32), 0.1, 1.9),
        "w_out": normal_values(key_of[9], (BLOCKS, HEADS, HD, D), WIDTH ** -0.5, 0.125, ((2, 64),)),
    }


epsilon = 1e-06

def project(scaled, weight, inv_rms):
    row_count = weight.shape[0] // N_DP
    total = jnp.zeros((scaled.shape[0], weight.shape[1]), jnp.float32)
    for part_index in range(N_DP):
        lo_row = part_index * row_count
        partial_value = jnp.dot(scaled[:, lo_row:lo_row + row_count], weight[lo_row:lo_row + row_count], preferred_element_type=jnp.float32)
        total = total + lax.optimization_barrier(partial_value.astype(jnp.bfloat16)).astype(jnp.float32)
    return (total * inv_rms).astype(jnp.bfloat16)

def reference(resid, norm_gain, w_query, w_forget, w_value, w_gate, gate_floor, states, out_gain, w_out):
    residual = resid
    batch = resid.shape[0]
    new_list = []
    for layer in range(BLOCKS):
        resid_f32 = residual.astype(jnp.float32)
        inv_rms = lax.rsqrt(lax.optimization_barrier(jnp.mean(resid_f32 * resid_f32, axis=1, keepdims=True)) + epsilon)
        scaled = (resid_f32 * norm_gain[layer]).astype(jnp.bfloat16)
        queries = project(scaled, w_query[layer], inv_rms)
        forget_pre = project(scaled, w_forget[layer], inv_rms)
        values = project(scaled, w_value[layer].reshape(D, WIDTH), inv_rms)
        gate_pre = project(scaled, w_gate[layer].reshape(D, WIDTH), inv_rms)
        floor_now = gate_floor[layer]
        keep = floor_now + (1.0 - floor_now) * jax.nn.sigmoid(forget_pre.astype(jnp.float32))
        keep = keep.reshape(batch, HEADS, HD)
        value_f32 = values.astype(jnp.float32).reshape(batch, HEADS, HD)
        state_new = keep[:, :, None, :] * states[layer] + (1.0 - keep)[:, :, None, :] * value_f32[:, :, :, None]
        query_f32 = queries.astype(jnp.float32).reshape(batch, HEADS, HD)
        readout = lax.optimization_barrier(jnp.sum(query_f32[:, :, None, :] * state_new, axis=3))
        mean_square = lax.optimization_barrier(jnp.mean(readout * readout, axis=2, keepdims=True))
        gate_f32 = gate_pre.astype(jnp.float32).reshape(batch, HEADS, HD)
        normed = (readout * lax.rsqrt(mean_square + epsilon) * out_gain[layer] * jax.nn.silu(gate_f32)).astype(jnp.bfloat16)
        branch = jnp.dot(normed.reshape(batch, WIDTH), w_out[layer].reshape(WIDTH, D), preferred_element_type=jnp.float32)
        residual = (residual.astype(jnp.float32) + branch).astype(jnp.bfloat16)
        new_list.append(state_new)
    return (residual, jnp.stack(new_list))
```

```python
import functools

import jax
import jax.numpy as jnp
from jax import lax
from jax.experimental import pallas as pl
from jax.experimental.pallas import tpu as pltpu
from jax.sharding import PartitionSpec as P

MESH = pl.DeviceIdType.MESH
EPS = 1e-06
F32, BF16 = jnp.float32, jnp.bfloat16
NZ, NY, NDP = 16, 4, 8
PITCH = 24


def lanes():
    return lax.broadcasted_iota(jnp.int32, (8, 128), 1)


def turn(parts):
    group = lax.broadcasted_iota(jnp.int32, parts[0].shape, parts[0].ndim - 1) // 32
    axis = parts[0].ndim - 1
    out = []
    for g in range(4):
        acc = parts[g]
        for p in range(4):
            if p != g:
                acc = jnp.where(group == p, pltpu.roll(parts[p], (32 * (p - g)) % 128, axis), acc)
        out.append(acc)
    return out


def kernel(
    x_ref, gain_ref, wt_ref, floor_ref, og_ref, wo_ref, st_hbm,
    xo_ref, so_hbm,
    gx, gq, gg, gr, wt, wo, st, kq, xs, xres, x1b,
    sx, rx, sw, rw, so_s, so_r, lsem,
):
    tp = lax.axis_index("tp")
    dp = lax.axis_index("dp")
    z, y = tp // NY, tp % NY
    core = dp % 2
    zdist = (8, 7, 9, 6, 10, 5, 11, 4, 12, 3, 13, 2, 14, 1, 15)
    zi = [lax.rem(z + k, NZ) for k in zdist]
    zp = [{"tp": i * NY + y} for i in zi]
    yp = [{"tp": z * NY + lax.rem(y + k, NY)} for k in (2, 1, 3)]
    dpp = [{"dp": lax.rem(dp + k, NDP)} for k in (4, 3, 5, 2, 6, 1, 7)]
    mate = {"dp": dp + 1 - 2 * core}

    loads = [pltpu.make_async_copy(st_hbm.at[b], st.at[b], lsem.at[b]) for b in range(2)]
    for c in loads:
        c.start()

    bar = pltpu.get_barrier_semaphore()
    for p in zp + yp + dpp:
        pl.semaphore_signal(bar, inc=1, device_id=p, device_id_type=MESH)
    gx[0, y, z, 0] = x_ref[...]
    pl.semaphore_wait(bar, len(zp) + len(yp) + len(dpp))

    def send(src, dst, s, r, p):
        pltpu.make_async_remote_copy(src, dst, s, r, device_id=p, device_id_type=MESH).start()

    def arrived(ref, s, r):
        pltpu.make_async_remote_copy(ref, ref, s, r, device_id=mate, device_id_type=MESH).wait_recv()

    def left(ref, s, r):
        pltpu.make_async_remote_copy(ref, ref, s, r, device_id=mate, device_id_type=MESH).wait_send()

    def z_send(buf, i):
        for p in zp:
            send(buf.at[y, z], buf.at[y, z], sx.at[i, 0], rx.at[i, 0], p)

    def z_wait(buf, i):
        arrived(buf.at[0, pl.ds(0, NZ - 1)], sx.at[i, 0], rx.at[i, 0])

    def y_send(buf, i):
        for p in yp:
            send(buf.at[y], buf.at[y], sx.at[i, 1], rx.at[i, 1], p)

    def y_wait(buf, i):
        arrived(buf.at[pl.ds(0, NY - 1)], sx.at[i, 1], rx.at[i, 1])

    def all_left(buf, i):
        left(buf.at[0, pl.ds(0, NZ - 1)], sx.at[i, 0], rx.at[i, 0])
        left(buf.at[pl.ds(0, NY - 1)], sx.at[i, 1], rx.at[i, 1])

    z_send(gx.at[0], 0)
    for b in range(2):
        for p in dpp:
            send(wt_ref.at[b], wt.at[b, dp], sw.at[b], rw.at[b], p)
    for i, p in zip(zi, zp):
        send(wo_ref.at[core, i], wo.at[core, z, y], so_s.at[0], so_r.at[0], p)
    for b in range(2):
        wt[b, dp] = wt_ref[b]
    wo[core, z, y] = wo_ref[core, z]
    z_wait(gx.at[0], 0)
    y_send(gx.at[0], 0)
    arrived(wt.at[0, pl.ds(0, NDP - 1)], sw.at[0], rw.at[0])
    y_wait(gx.at[0], 0)

    for b in range(2):
        base = 4 * b
        if b == 0:
            tiles = turn([gx[0, i, :, 0].astype(F32) for i in range(NY)])
            for a in range(4):
                for k in range(NZ):
                    xres[k, 8 * a : 8 * a + 8, :] = tiles[a][k]
        else:
            tiles = [gx[1, a, :, 0].astype(F32) for a in range(NY)]
        inv = []
        for a in range(4):
            sq = jnp.sum(jnp.sum(tiles[a] * tiles[a], axis=0), axis=1, keepdims=True)
            inv.append(lax.rsqrt(sq / (NZ * 128) + EPS))
            for k in range(NZ):
                scaled = tiles[a][k] * gain_ref[b : b + 1, 128 * k : 128 * k + 128]
                xs[8 * a : 8 * a + 8, 128 * k : 128 * k + 128] = scaled.astype(BF16)
        inv = jnp.concatenate(inv, axis=0)
        if b == 1:
            arrived(wt.at[1, pl.ds(0, NDP - 1)], sw.at[1], rw.at[1])
        total = jnp.zeros((32, 128), F32)
        for d in range(NDP):
            part = lax.dot_general(
                xs[:, 256 * d : 256 * d + 256], wt[b, d], (((1,), (1,)), ((), ())), preferred_element_type=F32
            )
            total = total + part.astype(BF16).astype(F32)
        proj = (total * inv).astype(BF16).astype(F32)
        packed = turn([proj[8 * a : 8 * a + 8] for a in range(4)])
        gq[b, y, z, 0] = packed[0].astype(BF16)
        gq[b, y, z, 1] = packed[1].astype(BF16)
        z_send(gq.at[b], base + 1)
        gate = packed[3]
        gg[b, y, z, 0] = (og_ref[b : b + 1, :] * (gate / (1.0 + jnp.exp(-gate)))).astype(BF16)
        z_send(gg.at[b], base + 2)
        if b == 0:
            arrived(wo.at[0, pl.ds(0, NZ - 1), 0], so_s.at[0], so_r.at[0])
            for p in yp:
                send(wo.at[core, :, y], wo.at[core, :, y], so_s.at[1], so_r.at[1], p)
        vt = jnp.transpose(jnp.concatenate([proj, jnp.zeros((96, 128), F32)], axis=0))
        z_wait(gq.at[b], base + 1)
        y_send(gq.at[b], base + 1)
        z_wait(gg.at[b], base + 2)
        y_send(gg.at[b], base + 2)
        y_wait(gq.at[b], base + 1)
        forget = turn([gq[b, i, :, 1].astype(F32) for i in range(NY)])
        query = turn([gq[b, i, :, 0].astype(F32) for i in range(NY)])
        for a in range(4):
            for k in range(NZ):
                low = floor_ref[b : b + 1, 128 * k : 128 * k + 128]
                keep = low + (1.0 - low) * (1.0 / (1.0 + jnp.exp(-forget[a][k])))
                kq[0, pl.ds(8 * a * PITCH + k, 8, stride=PITCH), :] = keep
                kq[1, pl.ds(8 * a * PITCH + k, 8, stride=PITCH), :] = query[a][k]
        loads[b].wait()
        lane = lanes()
        read = [[jnp.zeros((8, 128), F32) for _ in range(2)] for _ in range(2)]
        for s in range(32):
            for hh in range(2):
                keep = kq[0, s * PITCH + 8 * hh : s * PITCH + 8 * hh + 8, :]
                quer = kq[1, s * PITCH + 8 * hh : s * PITCH + 8 * hh + 8, :]
                rest = 1.0 - keep
                for j in range(2):
                    rows = pl.ds(s * 32 + hh * 16 + j, 8, stride=2)
                    row0 = 64 + j * 16 + hh * 8
                    new = keep * st[b, rows, :] + rest * vt[row0 : row0 + 8, s : s + 1]
                    st[b, rows, :] = new
                    red = jnp.sum(quer * new, axis=1, keepdims=True)
                    read[j][hh] = jnp.where(lane == s, red, read[j][hh])
        rt = jnp.concatenate([read[0][0], read[0][1], read[1][0], read[1][1], jnp.zeros((96, 128), F32)], axis=0)
        rt = jnp.transpose(rt)
        tile = rt[0:8]
        for a in range(1, 4):
            tile = tile + pltpu.roll(rt[8 * a : 8 * a + 8], 32 * a, 1)
        gr[b, y, z, 0] = tile.astype(BF16)
        z_send(gr.at[b], base + 3)
        store = pltpu.make_async_copy(st.at[b], so_hbm.at[b], lsem.at[2 + b])
        store.start()
        if b == 0:
            first_store = store
            arrived(wo.at[0, pl.ds(0, NZ), pl.ds(0, NY - 1)], so_s.at[1], so_r.at[1])
            send(wo.at[core], wo.at[core], so_s.at[2], so_r.at[2], mate)
        y_wait(gg.at[b], base + 2)
        gate = turn([gg[b, i, :, 0].astype(F32) for i in range(NY)])
        z_wait(gr.at[b], base + 3)
        y_send(gr.at[b], base + 3)
        y_wait(gr.at[b], base + 3)
        read = turn([gr[b, i, :, 0].astype(F32) for i in range(NY)])
        for a in range(4):
            sq = jnp.sum(read[a] * read[a], axis=0)
            for shift in (64, 32, 16):
                sq = sq + pltpu.roll(sq, shift, 1)
            scale = lax.rsqrt(sq / 128.0 + EPS)
            for k in range(NZ):
                xs[8 * a : 8 * a + 8, 128 * k : 128 * k + 128] = (read[a][k] * scale * gate[a][k]).astype(BF16)
        if b == 0:
            arrived(wo.at[0], so_s.at[2], so_r.at[2])
        branch = jnp.dot(xs[...], wo[b].reshape(2048, 128), preferred_element_type=F32)
        if b == 0:
            fresh = (xres[z] + branch).astype(BF16).astype(F32)
            xres[0] = fresh
            for a in range(4):
                x1b[a] = fresh[8 * a : 8 * a + 8].astype(BF16)
            gx[1, y, z, 0] = x1b[y]
            z_send(gx.at[1], 4)
            z_wait(gx.at[1], 4)
            y_send(gx.at[1], 4)
            y_wait(gx.at[1], 4)
        else:
            fresh = xres[0] + branch
            mine = fresh
            for k in range(1, NY):
                mine = jnp.where(y == k, pltpu.roll(fresh, 128 - 32 * k, 1), mine)
            xo_ref[...] = mine[:, :32].astype(BF16)

    for b in range(2):
        all_left(gx.at[b], 4 * b)
        all_left(gq.at[b], 4 * b + 1)
        all_left(gg.at[b], 4 * b + 2)
        all_left(gr.at[b], 4 * b + 3)
        left(wt.at[b, pl.ds(0, NDP - 1)], sw.at[b], rw.at[b])
    left(wo.at[0, pl.ds(0, NZ - 1), 0], so_s.at[0], so_r.at[0])
    left(wo.at[0, pl.ds(0, NZ), pl.ds(0, NY - 1)], so_s.at[1], so_r.at[1])
    left(wo.at[0], so_s.at[2], so_r.at[2])
    first_store.wait()
    store.wait()


def shards(
    resid, norm_gain, w_query, w_forget, w_value, w_gate, gate_floor, states, out_gain, w_out
):
    seqs = resid.shape[0]
    x = resid.reshape(4, 8, 32).transpose(1, 0, 2).reshape(8, 128)
    value_t = w_value.transpose(0, 3, 2, 1).reshape(2, 32, 256)
    gate_t = w_gate.transpose(0, 3, 2, 1).reshape(2, 32, 256)
    wt = jnp.concatenate([w_query.transpose(0, 2, 1), w_forget.transpose(0, 2, 1), value_t, gate_t], axis=1)
    og = jnp.tile(out_gain.transpose(0, 2, 1).reshape(2, 32), (1, 4))
    wo = w_out.transpose(0, 2, 1, 3).reshape(2, 32, 16, 128).transpose(0, 2, 1, 3)
    st = states.reshape(2, seqs * 32, 128)
    vmem = pl.BlockSpec(memory_space=pltpu.VMEM)
    hbm = pl.BlockSpec(memory_space=pl.ANY)
    dma = pltpu.SemaphoreType.DMA
    new_resid, new_states = pl.pallas_call(
        kernel,
        out_shape=(jax.ShapeDtypeStruct((32, 32), BF16), jax.ShapeDtypeStruct(st.shape, F32)),
        in_specs=[vmem] * 6 + [hbm],
        out_specs=(vmem, hbm),
        scratch_shapes=[
            pltpu.VMEM((2, NY, NZ, 1, 8, 128), BF16),
            pltpu.VMEM((2, NY, NZ, 2, 8, 128), BF16),
            pltpu.VMEM((2, NY, NZ, 1, 8, 128), BF16),
            pltpu.VMEM((2, NY, NZ, 1, 8, 128), BF16),
            pltpu.VMEM((2, NDP, 128, 256), BF16),
            pltpu.VMEM((2, NZ, NY, 32, 128), BF16),
            pltpu.VMEM((2, 1024, 128), F32),
            pltpu.VMEM((2, 32 * PITCH, 128), F32),
            pltpu.VMEM((32, 2048), BF16),
            pltpu.VMEM((NZ, 32, 128), F32),
            pltpu.VMEM((4, 8, 128), BF16),
            dma((8, 2)),
            dma((8, 2)),
            dma((2,)),
            dma((2,)),
            dma((3,)),
            dma((3,)),
            dma((4,)),
        ],
        compiler_params=pltpu.CompilerParams(collective_id=0, has_side_effects=True),
        name="blocks",
    )(x, norm_gain, wt, gate_floor, og, wo, st)
    return new_resid, new_states.reshape(states.shape)


def solution(mesh):
    return jax.shard_map(
        shards,
        mesh=mesh,
        in_specs=(
            P("dp", "tp"),
            P(),
            P(None, "dp", "tp"),
            P(None, "dp", "tp"),
            P(None, "dp", None, "tp"),
            P(None, "dp", None, "tp"),
            P(),
            P(None, "dp", None, "tp", None),
            P(None, None, "tp"),
            P(None, None, "tp", None),
        ),
        out_specs=(P("dp", "tp"), P(None, "dp", None, "tp", None)),
        check_vma=False,
    )
```

```python
import functools

import jax
import jax.numpy as jnp
from jax import lax
from jax.experimental import pallas as pl
from jax.experimental.pallas import tpu as pltpu
from jax.sharding import PartitionSpec as P

MESH = pl.DeviceIdType.MESH
EPS = 1e-06
F32, BF16 = jnp.float32, jnp.bfloat16
NZ, NY, NDP = 16, 4, 8
PITCH = 24


def lanes():
    return lax.broadcasted_iota(jnp.int32, (8, 128), 1)


def turn(parts):
    group = lax.broadcasted_iota(jnp.int32, parts[0].shape, parts[0].ndim - 1) // 32
    axis = parts[0].ndim - 1
    out = []
    for g in range(4):
        acc = parts[g]
        for p in range(4):
            if p != g:
                acc = jnp.where(group == p, pltpu.roll(parts[p], (32 * (p - g)) % 128, axis), acc)
        out.append(acc)
    return out


def kernel(
    x_ref, gain_ref, wq_ref, wf_ref, wv_ref, wg_ref, floor_ref, og_ref, wo_ref, st_hbm,
    xo_ref, st,
    gx, gq, gg, gr, wt, wo, wsrc, own, kq, xs, xres, x1b, vt,
    sx, rx, sw, rw, so_s, so_r, lsem,
):
    tp = lax.axis_index("tp")
    dp = lax.axis_index("dp")
    z, y = tp // NY, tp % NY
    core = dp % 2
    zdist = (8, 7, 9, 6, 10, 5, 11, 4, 12, 3, 13, 2, 14, 1, 15)
    zi = [lax.rem(z + k, NZ) for k in zdist]
    zp = [{"tp": i * NY + y} for i in zi]
    yp = [{"tp": z * NY + lax.rem(y + k, NY)} for k in (2, 1, 3)]
    dpp = [{"dp": lax.rem(dp + k, NDP)} for k in (4, 3, 5, 2, 6, 1, 7)]
    mate = {"dp": dp + 1 - 2 * core}

    loads = [pltpu.make_async_copy(st_hbm.at[b], st.at[b], lsem.at[b]) for b in range(2)]
    for c in loads:
        c.start()

    bar = pltpu.get_barrier_semaphore()
    for p in zp + yp + dpp:
        pl.semaphore_signal(bar, inc=1, device_id=p, device_id_type=MESH)
    x_in = x_ref[...].astype(F32)
    gx[0, y, z, 0] = jnp.concatenate([x_in[8 * a : 8 * a + 8] for a in range(4)], axis=1).astype(BF16)
    pl.semaphore_wait(bar, len(zp) + len(yp) + len(dpp))

    def send(src, dst, s, r, p):
        pltpu.make_async_remote_copy(src, dst, s, r, device_id=p, device_id_type=MESH).start()

    def arrived(ref, s, r):
        pltpu.make_async_remote_copy(ref, ref, s, r, device_id=mate, device_id_type=MESH).wait_recv()

    def left(ref, s, r):
        pltpu.make_async_remote_copy(ref, ref, s, r, device_id=mate, device_id_type=MESH).wait_send()

    def z_send(buf, i):
        for p in zp:
            send(buf.at[y, z], buf.at[y, z], sx.at[i, 0], rx.at[i, 0], p)

    def z_wait(buf, i):
        arrived(buf.at[0, pl.ds(0, NZ - 1)], sx.at[i, 0], rx.at[i, 0])

    def y_send(buf, i):
        for p in yp:
            send(buf.at[y], buf.at[y], sx.at[i, 1], rx.at[i, 1], p)

    def y_wait(buf, i):
        arrived(buf.at[pl.ds(0, NY - 1)], sx.at[i, 1], rx.at[i, 1])

    def all_left(buf, i):
        left(buf.at[0, pl.ds(0, NZ - 1)], sx.at[i, 0], rx.at[i, 0])
        left(buf.at[pl.ds(0, NY - 1)], sx.at[i, 1], rx.at[i, 1])

    z_send(gx.at[0], 0)
    for b in range(2):
        own[b, 0:32, :] = wq_ref[b]
        own[b, 32:64, :] = wf_ref[b]
        own[b, 64:96, :] = wv_ref[b].reshape(32, 256)
        own[b, 96:128, :] = wg_ref[b].reshape(32, 256)
        wt[b, dp] = own[b]
        for p in dpp:
            send(own.at[b], wt.at[b, dp], sw.at[b], rw.at[b], p)
    for k in range(NZ):
        wsrc[k] = wo_ref[core, :, :, 128 * k : 128 * k + 128].reshape(32, 128)
    wo[core, z, y] = wsrc[z]
    for i, p in zip(zi, zp):
        send(wsrc.at[i], wo.at[core, z, y], so_s.at[0], so_r.at[0], p)
    spot = lax.broadcasted_iota(jnp.int32, (16, 128), 1) % 32
    head = lax.broadcasted_iota(jnp.int32, (16, 128), 0)
    gains = []
    for b in range(2):
        row = jnp.zeros((1, 128), F32)
        for j in range(2):
            pick = jnp.where(spot == 2 * head + j, 1.0, 0.0)
            row = row + jnp.dot(og_ref[b, j : j + 1, :], pick, precision=lax.Precision.HIGHEST, preferred_element_type=F32)
        gains.append(row)
    z_wait(gx.at[0], 0)
    y_send(gx.at[0], 0)
    arrived(wt.at[0, pl.ds(0, NDP - 1)], sw.at[0], rw.at[0])
    y_wait(gx.at[0], 0)

    for b in range(2):
        base = 4 * b
        if b == 0:
            tiles = turn([gx[0, i, :, 0].astype(F32) for i in range(NY)])
            for a in range(4):
                for k in range(NZ):
                    xres[k, 8 * a : 8 * a + 8, :] = tiles[a][k]
        else:
            tiles = [gx[1, a, :, 0].astype(F32) for a in range(NY)]
        inv = []
        for a in range(4):
            sq = jnp.sum(jnp.sum(tiles[a] * tiles[a], axis=0), axis=1, keepdims=True)
            inv.append(lax.rsqrt(sq / (NZ * 128) + EPS))
            for k in range(NZ):
                scaled = tiles[a][k] * gain_ref[b : b + 1, 128 * k : 128 * k + 128]
                xs[8 * a : 8 * a + 8, 128 * k : 128 * k + 128] = scaled.astype(BF16)
        inv = jnp.concatenate(inv, axis=0)
        if b == 1:
            arrived(wt.at[1, pl.ds(0, NDP - 1)], sw.at[1], rw.at[1])
        total = jnp.zeros((32, 128), F32)
        for d in range(NDP):
            part = lax.dot_general(
                xs[:, 256 * d : 256 * d + 256], wt[b, d], (((1,), (1,)), ((), ())), preferred_element_type=F32
            )
            total = total + part.astype(BF16).astype(F32)
        proj = (total * inv).astype(BF16).astype(F32)
        packed = turn([proj[8 * a : 8 * a + 8] for a in range(4)])
        gq[b, y, z, 0] = packed[0].astype(BF16)
        gq[b, y, z, 1] = packed[1].astype(BF16)
        z_send(gq.at[b], base + 1)
        gate = packed[3]
        gg[b, y, z, 0] = (gains[b] * (gate / (1.0 + jnp.exp(-gate)))).astype(BF16)
        z_send(gg.at[b], base + 2)
        if b == 0:
            arrived(wo.at[0, pl.ds(0, NZ - 1), 0], so_s.at[0], so_r.at[0])
            for p in yp:
                send(wo.at[core, :, y], wo.at[core, :, y], so_s.at[1], so_r.at[1], p)
        vt[...] = jnp.transpose(jnp.concatenate([proj, jnp.zeros((96, 128), F32)], axis=0))
        z_wait(gq.at[b], base + 1)
        y_send(gq.at[b], base + 1)
        z_wait(gg.at[b], base + 2)
        y_send(gg.at[b], base + 2)
        y_wait(gq.at[b], base + 1)
        forget = turn([gq[b, i, :, 1].astype(F32) for i in range(NY)])
        query = turn([gq[b, i, :, 0].astype(F32) for i in range(NY)])
        for a in range(4):
            for k in range(NZ):
                low = floor_ref[b : b + 1, 128 * k : 128 * k + 128]
                keep = low + (1.0 - low) * (1.0 / (1.0 + jnp.exp(-forget[a][k])))
                kq[0, pl.ds(8 * a * PITCH + k, 8, stride=PITCH), :] = keep
                kq[1, pl.ds(8 * a * PITCH + k, 8, stride=PITCH), :] = query[a][k]
        loads[b].wait()
        lane = lanes()
        read = [[jnp.zeros((8, 128), F32) for _ in range(2)] for _ in range(2)]
        vals = [[vt[pl.ds(64 + 16 * hh + j, 8, stride=2), :] for hh in range(2)] for j in range(2)]
        for s in range(32):
            for hh in range(2):
                keep = kq[0, s * PITCH + 8 * hh : s * PITCH + 8 * hh + 8, :]
                quer = kq[1, s * PITCH + 8 * hh : s * PITCH + 8 * hh + 8, :]
                rest = 1.0 - keep
                for j in range(2):
                    rows = pl.ds(s * 32 + hh * 16 + j, 8, stride=2)
                    new = keep * st[b, rows, :] + rest * vals[j][hh][:, s : s + 1]
                    st[b, rows, :] = new
                    red = jnp.sum(quer * new, axis=1, keepdims=True)
                    read[j][hh] = jnp.where(lane == s, red, read[j][hh])
        vt[...] = jnp.zeros((128, 128), F32)
        for j in range(2):
            for hh in range(2):
                vt[pl.ds(16 * hh + j, 8, stride=2), :] = read[j][hh]
        rt = jnp.transpose(vt[...])
        tile = rt[0:8]
        for a in range(1, 4):
            tile = tile + pltpu.roll(rt[8 * a : 8 * a + 8], 32 * a, 1)
        gr[b, y * NZ + z] = tile.astype(BF16)
        for i in zi:
            for k in (2, 1, 3, 0):
                to = {"tp": i * NY + lax.rem(y + k, NY)}
                send(gr.at[b, y * NZ + z], gr.at[b, y * NZ + z], sx.at[base + 3, 0], rx.at[base + 3, 0], to)
        for p in yp:
            send(gr.at[b, y * NZ + z], gr.at[b, y * NZ + z], sx.at[base + 3, 0], rx.at[base + 3, 0], p)
        if b == 0:
            arrived(wo.at[0, pl.ds(0, NZ), pl.ds(0, NY - 1)], so_s.at[1], so_r.at[1])
            send(wo.at[core], wo.at[core], so_s.at[2], so_r.at[2], mate)
        y_wait(gg.at[b], base + 2)
        gate = turn([gg[b, i, :, 0].astype(F32) for i in range(NY)])
        arrived(gr.at[b, pl.ds(0, NY * NZ - 1)], sx.at[base + 3, 0], rx.at[base + 3, 0])
        read = turn([gr[b, NZ * i : NZ * i + NZ].astype(F32) for i in range(NY)])
        for a in range(4):
            sq = jnp.sum(read[a] * read[a], axis=0)
            for shift in (64, 32):
                sq = sq + pltpu.roll(sq, shift, 1)
            sq = sq + jnp.where(lane % 2 == 0, pltpu.roll(sq, 127, 1), pltpu.roll(sq, 1, 1))
            scale = lax.rsqrt(sq / 128.0 + EPS)
            for k in range(NZ):
                xs[8 * a : 8 * a + 8, 128 * k : 128 * k + 128] = (read[a][k] * scale * gate[a][k]).astype(BF16)
        if b == 0:
            arrived(wo.at[0], so_s.at[2], so_r.at[2])
        branch = jnp.dot(xs[...], wo[b].reshape(2048, 128), preferred_element_type=F32)
        if b == 0:
            fresh = (xres[z] + branch).astype(BF16).astype(F32)
            xres[0] = fresh
            for a in range(4):
                x1b[a] = fresh[8 * a : 8 * a + 8].astype(BF16)
            gx[1, y, z, 0] = x1b[y]
            z_send(gx.at[1], 4)
            z_wait(gx.at[1], 4)
            y_send(gx.at[1], 4)
            y_wait(gx.at[1], 4)
        else:
            fresh = xres[0] + branch
            mine = fresh
            for k in range(1, NY):
                mine = jnp.where(y == k, pltpu.roll(fresh, 128 - 32 * k, 1), mine)
            xo_ref[...] = mine[:, :32].astype(BF16)

    for b in range(2):
        all_left(gx.at[b], 4 * b)
        all_left(gq.at[b], 4 * b + 1)
        all_left(gg.at[b], 4 * b + 2)
        left(gr.at[b, pl.ds(0, NY * NZ - 1)], sx.at[4 * b + 3, 0], rx.at[4 * b + 3, 0])
        left(wt.at[b, pl.ds(0, NDP - 1)], sw.at[b], rw.at[b])
    left(wo.at[0, pl.ds(0, NZ - 1), 0], so_s.at[0], so_r.at[0])
    left(wo.at[0, pl.ds(0, NZ), pl.ds(0, NY - 1)], so_s.at[1], so_r.at[1])
    left(wo.at[0], so_s.at[2], so_r.at[2])


def shards(
    resid, norm_gain, w_query, w_forget, w_value, w_gate, gate_floor, states, out_gain, w_out
):
    st = states.reshape(2, resid.shape[0] * 32, 128)
    vmem = pl.BlockSpec(memory_space=pltpu.VMEM)
    hbm = pl.BlockSpec(memory_space=pl.ANY)
    dma = pltpu.SemaphoreType.DMA
    new_resid, new_states = pl.pallas_call(
        kernel,
        out_shape=(pltpu.VMEM((32, 32), BF16), pltpu.VMEM(st.shape, F32)),
        in_specs=[vmem] * 9 + [hbm],
        out_specs=(vmem, vmem),
        scratch_shapes=[
            pltpu.VMEM((2, NY, NZ, 1, 8, 128), BF16),
            pltpu.VMEM((2, NY, NZ, 2, 8, 128), BF16),
            pltpu.VMEM((2, NY, NZ, 1, 8, 128), BF16),
            pltpu.VMEM((2, NY * NZ, 8, 128), BF16),
            pltpu.VMEM((2, NDP, 128, 256), BF16),
            pltpu.VMEM((2, NZ, NY, 32, 128), BF16),
            pltpu.VMEM((NZ, 32, 128), BF16),
            pltpu.VMEM((2, 128, 256), BF16),
            pltpu.VMEM((2, 32 * PITCH, 128), F32),
            pltpu.VMEM((32, 2048), BF16),
            pltpu.VMEM((NZ, 32, 128), F32),
            pltpu.VMEM((4, 8, 128), BF16),
            pltpu.VMEM((128, 128), F32),
            dma((8, 2)),
            dma((8, 2)),
            dma((2,)),
            dma((2,)),
            dma((3,)),
            dma((3,)),
            dma((2,)),
        ],
        compiler_params=pltpu.CompilerParams(collective_id=0, has_side_effects=True),
        name="blocks",
    )(
        resid,
        norm_gain,
        w_query.transpose(0, 2, 1),
        w_forget.transpose(0, 2, 1),
        w_value.transpose(0, 2, 3, 1),
        w_gate.transpose(0, 2, 3, 1),
        gate_floor,
        out_gain.transpose(0, 2, 1),
        w_out,
        st,
    )
    return new_resid, new_states.reshape(states.shape)


def solution(mesh):
    return jax.shard_map(
        shards,
        mesh=mesh,
        in_specs=(
            P("dp", "tp"),
            P(),
            P(None, "dp", "tp"),
            P(None, "dp", "tp"),
            P(None, "dp", None, "tp"),
            P(None, "dp", None, "tp"),
            P(),
            P(None, "dp", None, "tp", None),
            P(None, None, "tp"),
            P(None, None, "tp", None),
        ),
        out_specs=(P("dp", "tp"), P(None, "dp", None, "tp", None)),
        check_vma=False,
    )
```

```python
import functools

import jax
import jax.numpy as jnp
from jax import lax
from jax.experimental import pallas as pl
from jax.experimental.pallas import tpu as pltpu
from jax.sharding import PartitionSpec as P

MESH = pl.DeviceIdType.MESH
EPS = 1e-06
F32, BF16 = jnp.float32, jnp.bfloat16
NZ, NY, NDP = 16, 4, 8
PITCH = 24


def lanes():
    return lax.broadcasted_iota(jnp.int32, (8, 128), 1)


def turn(parts):
    group = lax.broadcasted_iota(jnp.int32, parts[0].shape, parts[0].ndim - 1) // 32
    axis = parts[0].ndim - 1
    out = []
    for g in range(4):
        acc = parts[g]
        for p in range(4):
            if p != g:
                acc = jnp.where(group == p, pltpu.roll(parts[p], (32 * (p - g)) % 128, axis), acc)
        out.append(acc)
    return out


def kernel(
    x_ref, gain_ref, wq_ref, wf_ref, wv_ref, wg_ref, floor_ref, og_ref, wo_ref, st_hbm,
    xo_ref, st,
    x0, x1, gq, gg, gr, wt, wo, wsrc, own, kq, xs, xres, x1b, vt,
    sx, rx, sw, rw, so_s, so_r, lsem,
):
    tp = lax.axis_index("tp")
    dp = lax.axis_index("dp")
    z, y = tp // NY, tp % NY
    core = dp % 2
    zdist = (8, 7, 9, 6, 10, 5, 11, 4, 12, 3, 13, 2, 14, 1, 15)
    zclose = (4, -4, 3, -3, 2, -2, 1, -1)
    zi = [lax.rem(z + k, NZ) for k in zdist]
    zp = [{"tp": i * NY + y} for i in zi]
    yp = [{"tp": z * NY + lax.rem(y + k, NY)} for k in (2, 1, 3)]
    dpp = [{"dp": lax.rem(dp + k, NDP)} for k in (4, 3, 5, 2, 6, 1, 7)]
    mate = {"dp": dp + 1 - 2 * core}

    loads = [pltpu.make_async_copy(st_hbm.at[b], st.at[b], lsem.at[b]) for b in range(2)]
    for c in loads:
        c.start()

    bar = pltpu.get_barrier_semaphore()
    zc = [{"tp": lax.rem(z + NZ + k, NZ) * NY + y} for k in zclose]
    for p in zc + yp + dpp:
        pl.semaphore_signal(bar, inc=1, device_id=p, device_id_type=MESH)
    x_in = x_ref[...].astype(F32)
    x0[y, 8] = jnp.concatenate([x_in[8 * a : 8 * a + 8] for a in range(4)], axis=1).astype(BF16)
    pl.semaphore_wait(bar, len(zc) + len(yp) + len(dpp))

    def send(src, dst, s, r, p):
        pltpu.make_async_remote_copy(src, dst, s, r, device_id=p, device_id_type=MESH).start()

    def arrived(ref, s, r):
        pltpu.make_async_remote_copy(ref, ref, s, r, device_id=mate, device_id_type=MESH).wait_recv()

    def left(ref, s, r):
        pltpu.make_async_remote_copy(ref, ref, s, r, device_id=mate, device_id_type=MESH).wait_send()

    def z_send(buf, i):
        for p in zp:
            send(buf.at[y, z], buf.at[y, z], sx.at[i, 0], rx.at[i, 0], p)

    def z_wait(buf, i):
        arrived(buf.at[0, pl.ds(0, NZ - 1)], sx.at[i, 0], rx.at[i, 0])

    def y_send(buf, i):
        for p in yp:
            send(buf.at[y], buf.at[y], sx.at[i, 1], rx.at[i, 1], p)

    def y_wait(buf, i):
        arrived(buf.at[pl.ds(0, NY - 1)], sx.at[i, 1], rx.at[i, 1])

    def to_all(buf, i):
        tile = buf.at[y * NZ + z]
        for j in zi:
            for k in (2, 1, 3, 0):
                send(tile, tile, sx.at[i, 0], rx.at[i, 0], {"tp": j * NY + lax.rem(y + k, NY)})
        for p in yp:
            send(tile, tile, sx.at[i, 0], rx.at[i, 0], p)

    def all_here(buf, i):
        arrived(buf.at[pl.ds(0, NY * NZ - 1)], sx.at[i, 0], rx.at[i, 0])

    def all_left(buf, i):
        left(buf.at[0, pl.ds(0, NZ - 1)], sx.at[i, 0], rx.at[i, 0])
        left(buf.at[pl.ds(0, NY - 1)], sx.at[i, 1], rx.at[i, 1])

    for k, p in zip(zclose, zc):
        send(x0.at[y, 8], x0.at[y, 8 - k], sx.at[0, 0], rx.at[0, 0], p)
    for b in range(2):
        own[b, 0:32, :] = wq_ref[b]
        own[b, 32:64, :] = wf_ref[b]
        own[b, 64:96, :] = wv_ref[b].reshape(32, 256)
        own[b, 96:128, :] = wg_ref[b].reshape(32, 256)
        wt[b, dp] = own[b]
        for p in dpp:
            send(own.at[b], wt.at[b, dp], sw.at[b], rw.at[b], p)
    for k in range(NZ):
        wsrc[k] = wo_ref[core, :, :, 128 * k : 128 * k + 128].reshape(32, 128)
    wo[core, z, y] = wsrc[z]
    spot = lax.broadcasted_iota(jnp.int32, (16, 128), 1) % 32
    head = lax.broadcasted_iota(jnp.int32, (16, 128), 0)
    gains = []
    for b in range(2):
        row = jnp.zeros((1, 128), F32)
        for j in range(2):
            pick = jnp.where(spot == 2 * head + j, 1.0, 0.0)
            row = row + jnp.dot(og_ref[b, j : j + 1, :], pick, precision=lax.Precision.HIGHEST, preferred_element_type=F32)
        gains.append(row)
    arrived(x0.at[0, pl.ds(0, 8)], sx.at[0, 0], rx.at[0, 0])
    for k in (2, 1, 3, 0):
        yk = lax.rem(y + k, NY)
        up = {"tp": lax.rem(z + 4, NZ) * NY + yk}
        down = {"tp": lax.rem(z + NZ - 4, NZ) * NY + yk}
        send(x0.at[y, pl.ds(4, 4)], x0.at[y, pl.ds(0, 4)], sx.at[0, 1], rx.at[0, 1], up)
        send(x0.at[y, pl.ds(9, 3)], x0.at[y, pl.ds(13, 3)], sx.at[0, 1], rx.at[0, 1], down)
    for p in yp:
        send(x0.at[y, pl.ds(4, 9)], x0.at[y, pl.ds(4, 9)], sx.at[0, 1], rx.at[0, 1], p)
    for i, p in zip(zi, zp):
        send(wsrc.at[i], wo.at[core, z, y], so_s.at[0], so_r.at[0], p)
    arrived(wt.at[0, pl.ds(0, NDP - 1)], sw.at[0], rw.at[0])
    arrived(gr.at[0, pl.ds(0, 55)], sx.at[0, 1], rx.at[0, 1])

    for b in range(2):
        base = 4 * b
        if b == 0:
            tiles = [[], [], [], []]
            for k in range(NZ):
                slot = lax.rem(k + 24 - z, NZ)
                four = turn([x0[i, slot].astype(F32) for i in range(NY)])
                for a in range(4):
                    tiles[a].append(four[a])
                    xres[k, 8 * a : 8 * a + 8, :] = four[a]
            tiles = [jnp.stack(t) for t in tiles]
        else:
            tiles = [x1[NZ * a : NZ * a + NZ].astype(F32) for a in range(NY)]
        inv = []
        for a in range(4):
            sq = jnp.sum(jnp.sum(tiles[a] * tiles[a], axis=0), axis=1, keepdims=True)
            inv.append(lax.rsqrt(sq / (NZ * 128) + EPS))
            for k in range(NZ):
                scaled = tiles[a][k] * gain_ref[b : b + 1, 128 * k : 128 * k + 128]
                xs[8 * a : 8 * a + 8, 128 * k : 128 * k + 128] = scaled.astype(BF16)
        inv = jnp.concatenate(inv, axis=0)
        if b == 1:
            arrived(wt.at[1, pl.ds(0, NDP - 1)], sw.at[1], rw.at[1])
        total = jnp.zeros((32, 128), F32)
        for d in range(NDP):
            part = lax.dot_general(
                xs[:, 256 * d : 256 * d + 256], wt[b, d], (((1,), (1,)), ((), ())), preferred_element_type=F32
            )
            total = total + part.astype(BF16).astype(F32)
        proj = (total * inv).astype(BF16).astype(F32)
        packed = turn([proj[8 * a : 8 * a + 8] for a in range(4)])
        gq[b, y, z, 0] = packed[0].astype(BF16)
        gq[b, y, z, 1] = packed[1].astype(BF16)
        z_send(gq.at[b], base + 1)
        gate = packed[3]
        gg[b, y, z, 0] = (gains[b] * (gate / (1.0 + jnp.exp(-gate)))).astype(BF16)
        z_send(gg.at[b], base + 2)
        if b == 0:
            arrived(wo.at[0, pl.ds(0, NZ - 1), 0], so_s.at[0], so_r.at[0])
            for p in yp:
                send(wo.at[core, :, y], wo.at[core, :, y], so_s.at[1], so_r.at[1], p)
        vt[...] = jnp.transpose(jnp.concatenate([proj, jnp.zeros((96, 128), F32)], axis=0))
        z_wait(gq.at[b], base + 1)
        y_send(gq.at[b], base + 1)
        z_wait(gg.at[b], base + 2)
        y_send(gg.at[b], base + 2)
        y_wait(gq.at[b], base + 1)
        forget = turn([gq[b, i, :, 1].astype(F32) for i in range(NY)])
        query = turn([gq[b, i, :, 0].astype(F32) for i in range(NY)])
        for a in range(4):
            for k in range(NZ):
                low = floor_ref[b : b + 1, 128 * k : 128 * k + 128]
                keep = low + (1.0 - low) * (1.0 / (1.0 + jnp.exp(-forget[a][k])))
                kq[0, pl.ds(8 * a * PITCH + k, 8, stride=PITCH), :] = keep
                kq[1, pl.ds(8 * a * PITCH + k, 8, stride=PITCH), :] = query[a][k]
        loads[b].wait()
        lane = lanes()
        read = [[jnp.zeros((8, 128), F32) for _ in range(2)] for _ in range(2)]
        vals = [[vt[pl.ds(64 + 16 * hh + j, 8, stride=2), :] for hh in range(2)] for j in range(2)]
        for s in range(32):
            for hh in range(2):
                keep = kq[0, s * PITCH + 8 * hh : s * PITCH + 8 * hh + 8, :]
                quer = kq[1, s * PITCH + 8 * hh : s * PITCH + 8 * hh + 8, :]
                rest = 1.0 - keep
                for j in range(2):
                    rows = pl.ds(s * 32 + hh * 16 + j, 8, stride=2)
                    new = keep * st[b, rows, :] + rest * vals[j][hh][:, s : s + 1]
                    st[b, rows, :] = new
                    red = jnp.sum(quer * new, axis=1, keepdims=True)
                    read[j][hh] = jnp.where(lane == s, red, read[j][hh])
        vt[...] = jnp.zeros((128, 128), F32)
        for j in range(2):
            for hh in range(2):
                vt[pl.ds(16 * hh + j, 8, stride=2), :] = read[j][hh]
        rt = jnp.transpose(vt[...])
        tile = rt[0:8]
        for a in range(1, 4):
            tile = tile + pltpu.roll(rt[8 * a : 8 * a + 8], 32 * a, 1)
        gr[b, y * NZ + z] = tile.astype(BF16)
        to_all(gr.at[b], base + 3)
        if b == 0:
            arrived(wo.at[0, pl.ds(0, NZ), pl.ds(0, NY - 1)], so_s.at[1], so_r.at[1])
            send(wo.at[core], wo.at[core], so_s.at[2], so_r.at[2], mate)
        y_wait(gg.at[b], base + 2)
        gate = turn([gg[b, i, :, 0].astype(F32) for i in range(NY)])
        all_here(gr.at[b], base + 3)
        read = turn([gr[b, NZ * i : NZ * i + NZ].astype(F32) for i in range(NY)])
        for a in range(4):
            sq = jnp.sum(read[a] * read[a], axis=0)
            for shift in (64, 32):
                sq = sq + pltpu.roll(sq, shift, 1)
            sq = sq + jnp.where(lane % 2 == 0, pltpu.roll(sq, 127, 1), pltpu.roll(sq, 1, 1))
            scale = lax.rsqrt(sq / 128.0 + EPS)
            for k in range(NZ):
                xs[8 * a : 8 * a + 8, 128 * k : 128 * k + 128] = (read[a][k] * scale * gate[a][k]).astype(BF16)
        if b == 0:
            arrived(wo.at[0], so_s.at[2], so_r.at[2])
        branch = jnp.dot(xs[...], wo[b].reshape(2048, 128), preferred_element_type=F32)
        if b == 0:
            fresh = (xres[z] + branch).astype(BF16).astype(F32)
            xres[0] = fresh
            for a in range(4):
                x1b[a] = fresh[8 * a : 8 * a + 8].astype(BF16)
            x1[y * NZ + z] = x1b[y]
            to_all(x1, 4)
            all_here(x1, 4)
        else:
            fresh = xres[0] + branch
            mine = fresh
            for k in range(1, NY):
                mine = jnp.where(y == k, pltpu.roll(fresh, 128 - 32 * k, 1), mine)
            xo_ref[...] = mine[:, :32].astype(BF16)

    for b in range(2):
        all_left(gq.at[b], 4 * b + 1)
        all_left(gg.at[b], 4 * b + 2)
        left(gr.at[b, pl.ds(0, NY * NZ - 1)], sx.at[4 * b + 3, 0], rx.at[4 * b + 3, 0])
        left(wt.at[b, pl.ds(0, NDP - 1)], sw.at[b], rw.at[b])
    left(x0.at[0, pl.ds(0, 8)], sx.at[0, 0], rx.at[0, 0])
    left(gr.at[0, pl.ds(0, 55)], sx.at[0, 1], rx.at[0, 1])
    left(x1.at[pl.ds(0, NY * NZ - 1)], sx.at[4, 0], rx.at[4, 0])
    left(wo.at[0, pl.ds(0, NZ - 1), 0], so_s.at[0], so_r.at[0])
    left(wo.at[0, pl.ds(0, NZ), pl.ds(0, NY - 1)], so_s.at[1], so_r.at[1])
    left(wo.at[0], so_s.at[2], so_r.at[2])


def shards(
    resid, norm_gain, w_query, w_forget, w_value, w_gate, gate_floor, states, out_gain, w_out
):
    st = states.reshape(2, resid.shape[0] * 32, 128)
    vmem = pl.BlockSpec(memory_space=pltpu.VMEM)
    hbm = pl.BlockSpec(memory_space=pl.ANY)
    dma = pltpu.SemaphoreType.DMA
    new_resid, new_states = pl.pallas_call(
        kernel,
        out_shape=(pltpu.VMEM((32, 32), BF16), pltpu.VMEM(st.shape, F32)),
        in_specs=[vmem] * 9 + [hbm],
        out_specs=(vmem, vmem),
        scratch_shapes=[
            pltpu.VMEM((NY, NZ, 8, 128), BF16),
            pltpu.VMEM((NY * NZ, 8, 128), BF16),
            pltpu.VMEM((2, NY, NZ, 2, 8, 128), BF16),
            pltpu.VMEM((2, NY, NZ, 1, 8, 128), BF16),
            pltpu.VMEM((2, NY * NZ, 8, 128), BF16),
            pltpu.VMEM((2, NDP, 128, 256), BF16),
            pltpu.VMEM((2, NZ, NY, 32, 128), BF16),
            pltpu.VMEM((NZ, 32, 128), BF16),
            pltpu.VMEM((2, 128, 256), BF16),
            pltpu.VMEM((2, 32 * PITCH, 128), F32),
            pltpu.VMEM((32, 2048), BF16),
            pltpu.VMEM((NZ, 32, 128), F32),
            pltpu.VMEM((4, 8, 128), BF16),
            pltpu.VMEM((128, 128), F32),
            dma((8, 2)),
            dma((8, 2)),
            dma((2,)),
            dma((2,)),
            dma((3,)),
            dma((3,)),
            dma((2,)),
        ],
        compiler_params=pltpu.CompilerParams(collective_id=0, has_side_effects=True),
        name="blocks",
    )(
        resid,
        norm_gain,
        w_query.transpose(0, 2, 1),
        w_forget.transpose(0, 2, 1),
        w_value.transpose(0, 2, 3, 1),
        w_gate.transpose(0, 2, 3, 1),
        gate_floor,
        out_gain.transpose(0, 2, 1),
        w_out,
        st,
    )
    return new_resid, new_states.reshape(states.shape)


def solution(mesh):
    return jax.shard_map(
        shards,
        mesh=mesh,
        in_specs=(
            P("dp", "tp"),
            P(),
            P(None, "dp", "tp"),
            P(None, "dp", "tp"),
            P(None, "dp", None, "tp"),
            P(None, "dp", None, "tp"),
            P(),
            P(None, "dp", None, "tp", None),
            P(None, None, "tp"),
            P(None, None, "tp", None),
        ),
        out_specs=(P("dp", "tp"), P(None, "dp", None, "tp", None)),
        check_vma=False,
    )
```

```python
import functools

import jax
import jax.numpy as jnp
from jax import lax
from jax.experimental import pallas as pl
from jax.experimental.pallas import tpu as pltpu
from jax.sharding import PartitionSpec as P

MESH = pl.DeviceIdType.MESH
EPS = 1e-06
F32, BF16 = jnp.float32, jnp.bfloat16
NZ, NY, NDP = 16, 4, 8
PITCH = 24


def lanes():
    return lax.broadcasted_iota(jnp.int32, (8, 128), 1)


def turn(parts):
    group = lax.broadcasted_iota(jnp.int32, parts[0].shape, parts[0].ndim - 1) // 32
    axis = parts[0].ndim - 1
    out = []
    for g in range(4):
        acc = parts[g]
        for p in range(4):
            if p != g:
                acc = jnp.where(group == p, pltpu.roll(parts[p], (32 * (p - g)) % 128, axis), acc)
        out.append(acc)
    return out


def kernel(
    x_ref, gain_ref, wq_ref, wf_ref, wv_ref, wg_ref, floor_ref, og_ref, wo_ref, st_hbm,
    xo_ref, st,
    x0, x1, gq, gq1, gg, gr, wt, wide, wq1, wv1, wo, wsrc, own, kq, xs, xres, x1b, vt,
    sx, rx, sw, rw, so_s, so_r, lsem,
):
    tp = lax.axis_index("tp")
    dp = lax.axis_index("dp")
    z, y = tp // NY, tp % NY
    core = dp % 2
    zdist = (8, 7, 9, 6, 10, 5, 11, 4, 12, 3, 13, 2, 14, 1, 15)
    zclose = (4, -4, 3, -3, 2, -2, 1, -1)
    zi = [lax.rem(z + k, NZ) for k in zdist]
    zp = [{"tp": i * NY + y} for i in zi]
    yp = [{"tp": z * NY + lax.rem(y + k, NY)} for k in (2, 1, 3)]
    dpp = [{"dp": lax.rem(dp + k, NDP)} for k in (4, 3, 5, 2, 6, 1, 7)]
    mate = {"dp": dp + 1 - 2 * core}
    x = dp // 2
    xp = [{"dp": lax.rem(x + k, 4) * 2 + core} for k in (2, 1, 3)]
    cls, turnover = z % 4, z // 4

    loads = [pltpu.make_async_copy(st_hbm.at[b], st.at[b], lsem.at[b]) for b in range(2)]
    for c in loads:
        c.start()

    bar = pltpu.get_barrier_semaphore()
    zc = [{"tp": lax.rem(z + NZ + k, NZ) * NY + y} for k in zclose]
    for p in zc + yp + dpp:
        pl.semaphore_signal(bar, inc=1, device_id=p, device_id_type=MESH)
    x_in = x_ref[...].astype(F32)
    x0[y, 8] = jnp.concatenate([x_in[8 * a : 8 * a + 8] for a in range(4)], axis=1).astype(BF16)
    pl.semaphore_wait(bar, len(zc) + len(yp) + len(dpp))

    def send(src, dst, s, r, p):
        pltpu.make_async_remote_copy(src, dst, s, r, device_id=p, device_id_type=MESH).start()

    def arrived(ref, s, r):
        pltpu.make_async_remote_copy(ref, ref, s, r, device_id=mate, device_id_type=MESH).wait_recv()

    def left(ref, s, r):
        pltpu.make_async_remote_copy(ref, ref, s, r, device_id=mate, device_id_type=MESH).wait_send()

    def z_send(buf, i):
        for p in zp:
            send(buf.at[y, z], buf.at[y, z], sx.at[i, 0], rx.at[i, 0], p)

    def z_wait(buf, i):
        arrived(buf.at[0, pl.ds(0, NZ - 1)], sx.at[i, 0], rx.at[i, 0])

    def y_send(buf, i):
        for p in yp:
            send(buf.at[y], buf.at[y], sx.at[i, 1], rx.at[i, 1], p)

    def y_wait(buf, i):
        arrived(buf.at[pl.ds(0, NY - 1)], sx.at[i, 1], rx.at[i, 1])

    def to_all(buf, i):
        tile = buf.at[y * NZ + z]
        for j in zi:
            for k in (2, 1, 3, 0):
                send(tile, tile, sx.at[i, 0], rx.at[i, 0], {"tp": j * NY + lax.rem(y + k, NY)})
        for p in yp:
            send(tile, tile, sx.at[i, 0], rx.at[i, 0], p)

    def all_here(buf, i):
        arrived(buf.at[pl.ds(0, NY * NZ - 1)], sx.at[i, 0], rx.at[i, 0])

    def all_left(buf, i):
        left(buf.at[0, pl.ds(0, NZ - 1)], sx.at[i, 0], rx.at[i, 0])
        left(buf.at[pl.ds(0, NY - 1)], sx.at[i, 1], rx.at[i, 1])

    for k, p in zip(zclose, zc):
        send(x0.at[y, 8], x0.at[y, 8 - k], sx.at[0, 0], rx.at[0, 0], p)
    for b in range(2):
        own[b, 0:32, :] = wq_ref[b]
        own[b, 32:64, :] = wf_ref[b]
        own[b, 64:96, :] = wv_ref[b].reshape(32, 256)
        own[b, 96:128, :] = wg_ref[b].reshape(32, 256)
        if b == 0:
            wt[dp] = own[0]
            for p in dpp:
                send(own.at[0], wt.at[dp], sw.at[0], rw.at[0], p)
    wide[turnover] = own[1, 0:64, :]
    wv1[x, core] = own[1, 64:128, :]
    for k in range(NZ):
        wsrc[k] = wo_ref[core, :, :, 128 * k : 128 * k + 128].reshape(4, 8, 128)
    wo[core, z, y, x] = wsrc[z, x]
    spot = lax.broadcasted_iota(jnp.int32, (16, 128), 1) % 32
    head = lax.broadcasted_iota(jnp.int32, (16, 128), 0)
    gains = []
    for b in range(2):
        row = jnp.zeros((1, 128), F32)
        for j in range(2):
            pick = jnp.where(spot == 2 * head + j, 1.0, 0.0)
            row = row + jnp.dot(og_ref[b, j : j + 1, :], pick, precision=lax.Precision.HIGHEST, preferred_element_type=F32)
        gains.append(row)
    arrived(x0.at[0, pl.ds(0, 8)], sx.at[0, 0], rx.at[0, 0])
    for k in (2, 1, 3, 0):
        yk = lax.rem(y + k, NY)
        up = {"tp": lax.rem(z + 4, NZ) * NY + yk}
        down = {"tp": lax.rem(z + NZ - 4, NZ) * NY + yk}
        send(x0.at[y, pl.ds(4, 4)], x0.at[y, pl.ds(0, 4)], sx.at[0, 1], rx.at[0, 1], up)
        send(x0.at[y, pl.ds(9, 3)], x0.at[y, pl.ds(13, 3)], sx.at[0, 1], rx.at[0, 1], down)
    for p in yp:
        send(x0.at[y, pl.ds(4, 9)], x0.at[y, pl.ds(4, 9)], sx.at[0, 1], rx.at[0, 1], p)
    for i, p in zip(zi, zp):
        send(wsrc.at[i, x], wo.at[core, z, y, x], so_s.at[0], so_r.at[0], p)
    arrived(wt.at[pl.ds(0, NDP - 1)], sw.at[0], rw.at[0])
    arrived(gr.at[0, pl.ds(0, 55)], sx.at[0, 1], rx.at[0, 1])

    def project(weights, width, inv):
        total = jnp.zeros((32, width), F32)
        for d in range(NDP):
            part = lax.dot_general(
                xs[:, 256 * d : 256 * d + 256], weights(d), (((1,), (1,)), ((), ())), preferred_element_type=F32
            )
            total = total + part.astype(BF16).astype(F32)
        return (total * inv).astype(BF16).astype(F32)

    for b in range(2):
        base = 4 * b
        if b == 0:
            tiles = [[], [], [], []]
            for k in range(NZ):
                slot = lax.rem(k + 24 - z, NZ)
                four = turn([x0[i, slot].astype(F32) for i in range(NY)])
                for a in range(4):
                    tiles[a].append(four[a])
                    xres[k, 8 * a : 8 * a + 8, :] = four[a]
            tiles = [jnp.stack(t) for t in tiles]
        else:
            tiles = [x1[NZ * a : NZ * a + NZ].astype(F32) for a in range(NY)]
        inv = []
        for a in range(4):
            sq = jnp.sum(jnp.sum(tiles[a] * tiles[a], axis=0), axis=1, keepdims=True)
            inv.append(lax.rsqrt(sq / (NZ * 128) + EPS))
            for k in range(NZ):
                scaled = tiles[a][k] * gain_ref[b : b + 1, 128 * k : 128 * k + 128]
                xs[8 * a : 8 * a + 8, 128 * k : 128 * k + 128] = scaled.astype(BF16)
        inv = jnp.concatenate(inv, axis=0)
        if b == 0:
            proj = project(lambda d: wt[d], 128, inv)
            packed = turn([proj[8 * a : 8 * a + 8] for a in range(4)])
            gq[y, z, 0] = packed[0].astype(BF16)
            gq[y, z, 1] = packed[1].astype(BF16)
            z_send(gq, 1)
            gate = packed[3]
        else:
            arrived(wq1.at[:, 0], sw.at[4], rw.at[4])
            arrived(wv1.at[:, 0], sw.at[5], rw.at[5])
            proj = project(lambda d: wq1[d // 2, d % 2].reshape(256, 256), 256, inv)
            unit = (y * 4 + cls) * 4
            for half in range(2):
                packed = turn([proj[8 * a : 8 * a + 8, 128 * half : 128 * half + 128] for a in range(4)])
                for q in range(2):
                    gq1[unit + 2 * half + q, 0] = packed[2 * q].astype(BF16)
                    gq1[unit + 2 * half + q, 1] = packed[2 * q + 1].astype(BF16)
            for k, first, count in ((2, 2, 2), (-2, 0, 2), (1, 0, 4), (-1, 0, 4), (0, 0, 4)):
                for j in (2, 1, 3) if k == 0 else (2, 1, 3, 0):
                    to = {"tp": lax.rem(z + NZ + k, NZ) * NY + lax.rem(y + j, NY)}
                    part = gq1.at[pl.ds(unit + first, count)]
                    send(part, part, sx.at[5, 0], rx.at[5, 0], to)
            proj = jnp.concatenate([project(lambda d: wv1[d // 2, d % 2], 64, inv), jnp.zeros((32, 64), F32)], axis=1)
            gate = turn([proj[8 * a : 8 * a + 8] for a in range(4)])[1]
        gg[b, y, z, 0] = (gains[b] * (gate / (1.0 + jnp.exp(-gate)))).astype(BF16)
        if b == 1:
            z_send(gg.at[b], base + 2)
        else:
            arrived(gr.at[0, pl.ds(0, NZ - 1)], so_s.at[0], so_r.at[0])
            for p in yp:
                send(wo.at[core, :, y, x], wo.at[core, :, y, x], so_s.at[1], so_r.at[1], p)
        vt[...] = jnp.transpose(jnp.concatenate([proj, jnp.zeros((96, 128), F32)], axis=0))
        if b == 0:
            z_wait(gq, 1)
            y_send(gq, 1)
            z_send(gg.at[0], 2)
            for k in (8, 4, 12):
                to = {"tp": lax.rem(z + k, NZ) * NY + y}
                send(own.at[1, pl.ds(0, 64)], wide.at[turnover], sw.at[1], rw.at[1], to)
            arrived(gr.at[0, pl.ds(0, 48)], so_s.at[1], so_r.at[1])
            for p in xp:
                send(wo.at[core, :, :, x], wo.at[core, :, :, x], so_s.at[2], so_r.at[2], p)
            y_wait(gq, 1)
        else:
            arrived(gq1.at[pl.ds(0, 60)], sx.at[5, 0], rx.at[5, 0])
        for k in range(NZ):
            low = floor_ref[b : b + 1, 128 * k : 128 * k + 128]
            for p in range(2):
                if b == 0:
                    four = turn([gq[i, k, p].astype(F32) for i in range(NY)])
                else:
                    four = turn([gq1[(4 * i + k % 4) * 4 + k // 4, p].astype(F32) for i in range(NY)])
                for a in range(4):
                    rows = pl.ds(8 * a * PITCH + k, 8, stride=PITCH)
                    if p == 0:
                        kq[1, rows, :] = four[a]
                    else:
                        kq[0, rows, :] = low + (1.0 - low) * (1.0 / (1.0 + jnp.exp(-four[a])))
        loads[b].wait()
        lane = lanes()
        read = [[jnp.zeros((8, 128), F32) for _ in range(2)] for _ in range(2)]
        first = 64 if b == 0 else 0
        vals = [[vt[pl.ds(first + 16 * hh + j, 8, stride=2), :] for hh in range(2)] for j in range(2)]
        for s in range(32):
            for hh in range(2):
                keep = kq[0, s * PITCH + 8 * hh : s * PITCH + 8 * hh + 8, :]
                quer = kq[1, s * PITCH + 8 * hh : s * PITCH + 8 * hh + 8, :]
                rest = 1.0 - keep
                for j in range(2):
                    rows = pl.ds(s * 32 + hh * 16 + j, 8, stride=2)
                    new = keep * st[b, rows, :] + rest * vals[j][hh][:, s : s + 1]
                    st[b, rows, :] = new
                    red = jnp.sum(quer * new, axis=1, keepdims=True)
                    read[j][hh] = jnp.where(lane == s, red, read[j][hh])
        vt[...] = jnp.zeros((128, 128), F32)
        for j in range(2):
            for hh in range(2):
                vt[pl.ds(16 * hh + j, 8, stride=2), :] = read[j][hh]
        rt = jnp.transpose(vt[...])
        tile = rt[0:8]
        for a in range(1, 4):
            tile = tile + pltpu.roll(rt[8 * a : 8 * a + 8], 32 * a, 1)
        gr[b, y * NZ + z] = tile.astype(BF16)
        to_all(gr.at[b], base + 3)
        if b == 0:
            z_wait(gg.at[0], 2)
            y_send(gg.at[0], 2)
            arrived(wo.at[0, pl.ds(0, 12)], so_s.at[2], so_r.at[2])
            send(wo.at[core], wo.at[core], so_s.at[3], so_r.at[3], mate)
            arrived(wide.at[pl.ds(0, 3)], sw.at[1], rw.at[1])
            for p in xp:
                send(wide, wq1.at[x, core], sw.at[2], rw.at[2], p)
                send(own.at[1, pl.ds(64, 64)], wv1.at[x, core], sw.at[3], rw.at[3], p)
            wq1[x, core] = wide[...]
        else:
            z_wait(gg.at[1], 6)
            y_send(gg.at[1], 6)
        y_wait(gg.at[b], base + 2)
        gate = turn([gg[b, i, :, 0].astype(F32) for i in range(NY)])
        all_here(gr.at[b], base + 3)
        read = turn([gr[b, NZ * i : NZ * i + NZ].astype(F32) for i in range(NY)])
        for a in range(4):
            sq = jnp.sum(read[a] * read[a], axis=0)
            for shift in (64, 32):
                sq = sq + pltpu.roll(sq, shift, 1)
            sq = sq + jnp.where(lane % 2 == 0, pltpu.roll(sq, 127, 1), pltpu.roll(sq, 1, 1))
            scale = lax.rsqrt(sq / 128.0 + EPS)
            for k in range(NZ):
                xs[8 * a : 8 * a + 8, 128 * k : 128 * k + 128] = (read[a][k] * scale * gate[a][k]).astype(BF16)
        if b == 0:
            arrived(wo.at[0], so_s.at[3], so_r.at[3])
        branch = jnp.dot(xs[...], wo[b].reshape(2048, 128), preferred_element_type=F32)
        if b == 0:
            fresh = (xres[z] + branch).astype(BF16).astype(F32)
            xres[0] = fresh
            for a in range(4):
                x1b[a] = fresh[8 * a : 8 * a + 8].astype(BF16)
            x1[y * NZ + z] = x1b[y]
            to_all(x1, 4)
            arrived(wq1.at[pl.ds(0, 3), 0], sw.at[2], rw.at[2])
            arrived(wv1.at[pl.ds(0, 3), 0], sw.at[3], rw.at[3])
            send(wq1.at[:, core], wq1.at[:, core], sw.at[4], rw.at[4], mate)
            send(wv1.at[:, core], wv1.at[:, core], sw.at[5], rw.at[5], mate)
            all_here(x1, 4)
        else:
            fresh = xres[0] + branch
            mine = fresh
            for k in range(1, NY):
                mine = jnp.where(y == k, pltpu.roll(fresh, 128 - 32 * k, 1), mine)
            xo_ref[...] = mine[:, :32].astype(BF16)

    for b in range(2):
        all_left(gg.at[b], 4 * b + 2)
        left(gr.at[b, pl.ds(0, NY * NZ - 1)], sx.at[4 * b + 3, 0], rx.at[4 * b + 3, 0])
    all_left(gq, 1)
    left(gq1.at[pl.ds(0, 60)], sx.at[5, 0], rx.at[5, 0])
    left(x0.at[0, pl.ds(0, 8)], sx.at[0, 0], rx.at[0, 0])
    left(gr.at[0, pl.ds(0, 55)], sx.at[0, 1], rx.at[0, 1])
    left(x1.at[pl.ds(0, NY * NZ - 1)], sx.at[4, 0], rx.at[4, 0])
    left(wt.at[pl.ds(0, NDP - 1)], sw.at[0], rw.at[0])
    left(wide.at[pl.ds(0, 3)], sw.at[1], rw.at[1])
    left(wq1.at[pl.ds(0, 3), 0], sw.at[2], rw.at[2])
    left(wv1.at[pl.ds(0, 3), 0], sw.at[3], rw.at[3])
    left(wq1.at[:, 0], sw.at[4], rw.at[4])
    left(wv1.at[:, 0], sw.at[5], rw.at[5])
    left(gr.at[0, pl.ds(0, NZ - 1)], so_s.at[0], so_r.at[0])
    left(gr.at[0, pl.ds(0, 48)], so_s.at[1], so_r.at[1])
    left(wo.at[0, pl.ds(0, 12)], so_s.at[2], so_r.at[2])
    left(wo.at[0], so_s.at[3], so_r.at[3])


def shards(
    resid, norm_gain, w_query, w_forget, w_value, w_gate, gate_floor, states, out_gain, w_out
):
    st = states.reshape(2, resid.shape[0] * 32, 128)
    vmem = pl.BlockSpec(memory_space=pltpu.VMEM)
    hbm = pl.BlockSpec(memory_space=pl.ANY)
    dma = pltpu.SemaphoreType.DMA
    new_resid, new_states = pl.pallas_call(
        kernel,
        out_shape=(pltpu.VMEM((32, 32), BF16), pltpu.VMEM(st.shape, F32)),
        in_specs=[vmem] * 9 + [hbm],
        out_specs=(vmem, vmem),
        scratch_shapes=[
            pltpu.VMEM((NY, NZ, 8, 128), BF16),
            pltpu.VMEM((NY * NZ, 8, 128), BF16),
            pltpu.VMEM((NY, NZ, 2, 8, 128), BF16),
            pltpu.VMEM((NY * NZ, 2, 8, 128), BF16),
            pltpu.VMEM((2, NY, NZ, 1, 8, 128), BF16),
            pltpu.VMEM((2, NY * NZ, 8, 128), BF16),
            pltpu.VMEM((NDP, 128, 256), BF16),
            pltpu.VMEM((4, 64, 256), BF16),
            pltpu.VMEM((4, 2, 4, 64, 256), BF16),
            pltpu.VMEM((4, 2, 64, 256), BF16),
            pltpu.VMEM((2, NZ, NY, 4, 8, 128), BF16),
            pltpu.VMEM((NZ, 4, 8, 128), BF16),
            pltpu.VMEM((2, 128, 256), BF16),
            pltpu.VMEM((2, 32 * PITCH, 128), F32),
            pltpu.VMEM((32, 2048), BF16),
            pltpu.VMEM((NZ, 32, 128), F32),
            pltpu.VMEM((4, 8, 128), BF16),
            pltpu.VMEM((128, 128), F32),
            dma((8, 2)),
            dma((8, 2)),
            dma((6,)),
            dma((6,)),
            dma((4,)),
            dma((4,)),
            dma((2,)),
        ],
        compiler_params=pltpu.CompilerParams(collective_id=0, has_side_effects=True),
        name="blocks",
    )(
        resid,
        norm_gain,
        w_query.transpose(0, 2, 1),
        w_forget.transpose(0, 2, 1),
        w_value.transpose(0, 2, 3, 1),
        w_gate.transpose(0, 2, 3, 1),
        gate_floor,
        out_gain.transpose(0, 2, 1),
        w_out,
        st,
    )
    return new_resid, new_states.reshape(states.shape)


def solution(mesh):
    return jax.shard_map(
        shards,
        mesh=mesh,
        in_specs=(
            P("dp", "tp"),
            P(),
            P(None, "dp", "tp"),
            P(None, "dp", "tp"),
            P(None, "dp", None, "tp"),
            P(None, "dp", None, "tp"),
            P(),
            P(None, "dp", None, "tp", None),
            P(None, None, "tp"),
            P(None, None, "tp", None),
        ),
        out_specs=(P("dp", "tp"), P(None, "dp", None, "tp", None)),
        check_vma=False,
    )
```

```python
import functools

import jax
import jax.numpy as jnp
from jax import lax
from jax.experimental import pallas as pl
from jax.experimental.pallas import tpu as pltpu
from jax.sharding import PartitionSpec as P

MESH = pl.DeviceIdType.MESH
EPS = 1e-06
F32, BF16 = jnp.float32, jnp.bfloat16
NZ, NY, NDP = 16, 4, 8
PITCH = 24


def lanes():
    return lax.broadcasted_iota(jnp.int32, (8, 128), 1)


def turn(parts):
    group = lax.broadcasted_iota(jnp.int32, parts[0].shape, parts[0].ndim - 1) // 32
    axis = parts[0].ndim - 1
    out = []
    for g in range(4):
        acc = parts[g]
        for p in range(4):
            if p != g:
                acc = jnp.where(group == p, pltpu.roll(parts[p], (32 * (p - g)) % 128, axis), acc)
        out.append(acc)
    return out


def kernel(
    x_hbm, gain_hbm, wq_hbm, wf_hbm, wv_hbm, wg_hbm, floor_hbm, og_hbm, wo_hbm, st_hbm,
    xo_ref, st,
    x0, x1, gq, gq1, gg, gr, wt, wide, wq1, wv1, wo, wsrc, own, kq, xs, xres, x1b, vt,
    x_ref, gain_ref, wv_ref, wg_ref, floor_ref, og_ref, wo_ref,
    sx, rx, sw, rw, so_s, so_r, lsem,
):
    tp = lax.axis_index("tp")
    dp = lax.axis_index("dp")
    z, y = tp // NY, tp % NY
    core = dp % 2
    zdist = (8, 7, 9, 6, 10, 5, 11, 4, 12, 3, 13, 2, 14, 1, 15)
    zclose = (4, -4, 3, -3, 2, -2, 1, -1)
    zi = [lax.rem(z + k, NZ) for k in zdist]
    zp = [{"tp": i * NY + y} for i in zi]
    yp = [{"tp": z * NY + lax.rem(y + k, NY)} for k in (2, 1, 3)]
    dpp = [{"dp": lax.rem(dp + k, NDP)} for k in (4, 3, 5, 2, 6, 1, 7)]
    mate = {"dp": dp + 1 - 2 * core}
    x = dp // 2
    xp = [{"dp": lax.rem(x + k, 4) * 2 + core} for k in (2, 1, 3)]
    cls, turnover = z % 4, z // 4

    bar = pltpu.get_barrier_semaphore()
    zc = [{"tp": lax.rem(z + NZ + k, NZ) * NY + y} for k in zclose]
    for p in zc + yp + dpp:
        pl.semaphore_signal(bar, inc=1, device_id=p, device_id_type=MESH)
    def load(src, dst, i):
        copy = pltpu.make_async_copy(src, dst, lsem.at[i])
        copy.start()
        return copy

    x_load = load(x_hbm, x_ref, 0)
    weight_loads = [
        load(wq_hbm, own.at[:, pl.ds(0, 32)], 1),
        load(wf_hbm, own.at[:, pl.ds(32, 32)], 2),
        load(wv_hbm, wv_ref, 3),
        load(wg_hbm, wg_ref, 4),
    ]
    small_loads = [
        load(wo_hbm.at[core], wo_ref, 5),
        load(gain_hbm, gain_ref, 6),
        load(floor_hbm, floor_ref, 7),
        load(og_hbm, og_ref, 8),
    ]
    loads = [load(st_hbm.at[b], st.at[b], 9 + b) for b in range(2)]
    x_load.wait()
    x_in = x_ref[...].astype(F32)
    x0[y, 8] = jnp.concatenate([x_in[8 * a : 8 * a + 8] for a in range(4)], axis=1).astype(BF16)
    pl.semaphore_wait(bar, len(zc) + len(yp) + len(dpp))

    def send(src, dst, s, r, p):
        pltpu.make_async_remote_copy(src, dst, s, r, device_id=p, device_id_type=MESH).start()

    def arrived(ref, s, r):
        pltpu.make_async_remote_copy(ref, ref, s, r, device_id=mate, device_id_type=MESH).wait_recv()

    def left(ref, s, r):
        pltpu.make_async_remote_copy(ref, ref, s, r, device_id=mate, device_id_type=MESH).wait_send()

    def z_send(buf, i):
        for p in zp:
            send(buf.at[y, z], buf.at[y, z], sx.at[i, 0], rx.at[i, 0], p)

    def z_wait(buf, i):
        arrived(buf.at[0, pl.ds(0, NZ - 1)], sx.at[i, 0], rx.at[i, 0])

    def y_send(buf, i):
        for p in yp:
            send(buf.at[y], buf.at[y], sx.at[i, 1], rx.at[i, 1], p)

    def y_wait(buf, i):
        arrived(buf.at[pl.ds(0, NY - 1)], sx.at[i, 1], rx.at[i, 1])

    def to_all(buf, i):
        tile = buf.at[y * NZ + z]
        for j in zi:
            for k in (2, 1, 3, 0):
                send(tile, tile, sx.at[i, 0], rx.at[i, 0], {"tp": j * NY + lax.rem(y + k, NY)})
        for p in yp:
            send(tile, tile, sx.at[i, 0], rx.at[i, 0], p)

    def all_here(buf, i):
        arrived(buf.at[pl.ds(0, NY * NZ - 1)], sx.at[i, 0], rx.at[i, 0])

    def all_left(buf, i):
        left(buf.at[0, pl.ds(0, NZ - 1)], sx.at[i, 0], rx.at[i, 0])
        left(buf.at[pl.ds(0, NY - 1)], sx.at[i, 1], rx.at[i, 1])

    for k, p in zip(zclose, zc):
        send(x0.at[y, 8], x0.at[y, 8 - k], sx.at[0, 0], rx.at[0, 0], p)
    for copy in weight_loads:
        copy.wait()
    for b in range(2):
        own[b, 64:96, :] = wv_ref[b].reshape(32, 256)
        own[b, 96:128, :] = wg_ref[b].reshape(32, 256)
        if b == 0:
            wt[dp] = own[0]
            for p in dpp:
                send(own.at[0], wt.at[dp], sw.at[0], rw.at[0], p)
    for copy in small_loads:
        copy.wait()
    wide[turnover] = own[1, 0:64, :]
    wv1[x, core] = own[1, 64:128, :]
    for k in range(NZ):
        wsrc[k] = wo_ref[:, :, 128 * k : 128 * k + 128].reshape(4, 8, 128)
    wo[core, z, y, x] = wsrc[z, x]
    spot = lax.broadcasted_iota(jnp.int32, (16, 128), 1) % 32
    head = lax.broadcasted_iota(jnp.int32, (16, 128), 0)
    gains = []
    for b in range(2):
        row = jnp.zeros((1, 128), F32)
        for j in range(2):
            pick = jnp.where(spot == 2 * head + j, 1.0, 0.0)
            row = row + jnp.dot(og_ref[b, j : j + 1, :], pick, precision=lax.Precision.HIGHEST, preferred_element_type=F32)
        gains.append(row)
    arrived(x0.at[0, pl.ds(0, 8)], sx.at[0, 0], rx.at[0, 0])
    for k in (2, 1, 3, 0):
        yk = lax.rem(y + k, NY)
        up = {"tp": lax.rem(z + 4, NZ) * NY + yk}
        down = {"tp": lax.rem(z + NZ - 4, NZ) * NY + yk}
        send(x0.at[y, pl.ds(4, 4)], x0.at[y, pl.ds(0, 4)], sx.at[0, 1], rx.at[0, 1], up)
        send(x0.at[y, pl.ds(9, 3)], x0.at[y, pl.ds(13, 3)], sx.at[0, 1], rx.at[0, 1], down)
    for p in yp:
        send(x0.at[y, pl.ds(4, 9)], x0.at[y, pl.ds(4, 9)], sx.at[0, 1], rx.at[0, 1], p)
    for i, p in zip(zi, zp):
        send(wsrc.at[i, x], wo.at[core, z, y, x], so_s.at[0], so_r.at[0], p)
    arrived(wt.at[pl.ds(0, NDP - 1)], sw.at[0], rw.at[0])
    arrived(gr.at[0, pl.ds(0, 55)], sx.at[0, 1], rx.at[0, 1])

    def project(weights, width, inv):
        total = jnp.zeros((32, width), F32)
        for d in range(NDP):
            part = lax.dot_general(
                xs[:, 256 * d : 256 * d + 256], weights(d), (((1,), (1,)), ((), ())), preferred_element_type=F32
            )
            total = total + part.astype(BF16).astype(F32)
        return (total * inv).astype(BF16).astype(F32)

    for b in range(2):
        base = 4 * b
        if b == 0:
            tiles = [[], [], [], []]
            for k in range(NZ):
                slot = lax.rem(k + 24 - z, NZ)
                four = turn([x0[i, slot].astype(F32) for i in range(NY)])
                for a in range(4):
                    tiles[a].append(four[a])
                    xres[k, 8 * a : 8 * a + 8, :] = four[a]
            tiles = [jnp.stack(t) for t in tiles]
        else:
            tiles = [x1[NZ * a : NZ * a + NZ].astype(F32) for a in range(NY)]
        inv = []
        for a in range(4):
            sq = jnp.sum(jnp.sum(tiles[a] * tiles[a], axis=0), axis=1, keepdims=True)
            inv.append(lax.rsqrt(sq / (NZ * 128) + EPS))
            for k in range(NZ):
                scaled = tiles[a][k] * gain_ref[b : b + 1, 128 * k : 128 * k + 128]
                xs[8 * a : 8 * a + 8, 128 * k : 128 * k + 128] = scaled.astype(BF16)
        inv = jnp.concatenate(inv, axis=0)
        if b == 0:
            proj = project(lambda d: wt[d], 128, inv)
            packed = turn([proj[8 * a : 8 * a + 8] for a in range(4)])
            gq[y, 8, 0] = packed[0].astype(BF16)
            gq[y, 8, 1] = packed[1].astype(BF16)
            for k in (8, 7, -7, 6, -6, 5, -5, 4, -4, 3, -3, 2, -2, 1, -1):
                to = {"tp": lax.rem(z + NZ + k, NZ) * NY + y}
                side = 0 if abs(k) > 4 else 2
                send(gq.at[y, 8], gq.at[y, 8 - k], sx.at[1, side], rx.at[1, side], to)
            gate = packed[3]
        else:
            arrived(wq1.at[:, 0], sw.at[4], rw.at[4])
            arrived(wv1.at[:, 0], sw.at[5], rw.at[5])
            proj = project(lambda d: wq1[d // 2, d % 2].reshape(256, 256), 256, inv)
            unit = (y * 4 + cls) * 4
            for half in range(2):
                packed = turn([proj[8 * a : 8 * a + 8, 128 * half : 128 * half + 128] for a in range(4)])
                for q in range(2):
                    gq1[unit + 2 * half + q, 0] = packed[2 * q].astype(BF16)
                    gq1[unit + 2 * half + q, 1] = packed[2 * q + 1].astype(BF16)
            for k, first, count in ((2, 2, 2), (-2, 0, 2), (1, 0, 4), (-1, 0, 4), (0, 0, 4)):
                for j in (2, 1, 3) if k == 0 else (2, 1, 3, 0):
                    to = {"tp": lax.rem(z + NZ + k, NZ) * NY + lax.rem(y + j, NY)}
                    part = gq1.at[pl.ds(unit + first, count)]
                    send(part, part, sx.at[5, 0], rx.at[5, 0], to)
            proj = jnp.concatenate([project(lambda d: wv1[d // 2, d % 2], 64, inv), jnp.zeros((32, 64), F32)], axis=1)
            gate = turn([proj[8 * a : 8 * a + 8] for a in range(4)])[1]
        gg[b, y, z, 0] = (gains[b] * (gate / (1.0 + jnp.exp(-gate)))).astype(BF16)
        if b == 1:
            z_send(gg.at[b], base + 2)
        else:
            arrived(gr.at[0, pl.ds(0, NZ - 1)], so_s.at[0], so_r.at[0])
            for p in yp:
                send(wo.at[core, :, y, x], wo.at[core, :, y, x], so_s.at[1], so_r.at[1], p)
        vt[...] = jnp.transpose(jnp.concatenate([proj, jnp.zeros((96, 128), F32)], axis=0))
        if b == 0:
            arrived(gq.at[0, pl.ds(0, 8)], sx.at[1, 2], rx.at[1, 2])
            for p in yp:
                send(gq.at[y, pl.ds(4, 9)], gq.at[y, pl.ds(4, 9)], sx.at[1, 1], rx.at[1, 1], p)
            z_send(gg.at[0], 2)
            arrived(gq.at[0, pl.ds(0, 7)], sx.at[1, 0], rx.at[1, 0])
            for p in yp:
                send(gq.at[y, pl.ds(0, 4)], gq.at[y, pl.ds(0, 4)], sx.at[1, 1], rx.at[1, 1], p)
                send(gq.at[y, pl.ds(13, 3)], gq.at[y, pl.ds(13, 3)], sx.at[1, 1], rx.at[1, 1], p)
            for k in (8, 4, 12):
                to = {"tp": lax.rem(z + k, NZ) * NY + y}
                send(own.at[1, pl.ds(0, 64)], wide.at[turnover], sw.at[1], rw.at[1], to)
            arrived(gr.at[0, pl.ds(0, 48)], so_s.at[1], so_r.at[1])
            for p in xp:
                send(wo.at[core, :, :, x], wo.at[core, :, :, x], so_s.at[2], so_r.at[2], p)
            y_wait(gq, 1)
        else:
            arrived(gq1.at[pl.ds(0, 60)], sx.at[5, 0], rx.at[5, 0])
        for k in range(NZ):
            low = floor_ref[b : b + 1, 128 * k : 128 * k + 128]
            for p in range(2):
                if b == 0:
                    four = turn([gq[i, lax.rem(k + 24 - z, NZ), p].astype(F32) for i in range(NY)])
                else:
                    four = turn([gq1[(4 * i + k % 4) * 4 + k // 4, p].astype(F32) for i in range(NY)])
                for a in range(4):
                    rows = pl.ds(8 * a * PITCH + k, 8, stride=PITCH)
                    if p == 0:
                        kq[1, rows, :] = four[a]
                    else:
                        kq[0, rows, :] = low + (1.0 - low) * (1.0 / (1.0 + jnp.exp(-four[a])))
        loads[b].wait()
        if b == 0:
            z_wait(gg.at[0], 2)
            y_send(gg.at[0], 2)
        lane = lanes()
        ones = jnp.ones((128, 128), BF16)
        read = [[jnp.zeros((8, 128), F32) for _ in range(2)] for _ in range(2)]
        first = 64 if b == 0 else 0
        vals = [[vt[pl.ds(first + 16 * hh + j, 8, stride=2), :] for hh in range(2)] for j in range(2)]
        for s0 in range(0, 32, 16):
            terms = [[[], []], [[], []]]
            for s in range(s0, s0 + 16):
                for hh in range(2):
                    keep = kq[0, s * PITCH + 8 * hh : s * PITCH + 8 * hh + 8, :]
                    quer = kq[1, s * PITCH + 8 * hh : s * PITCH + 8 * hh + 8, :]
                    rest = 1.0 - keep
                    for j in range(2):
                        rows = pl.ds(s * 32 + hh * 16 + j, 8, stride=2)
                        new = keep * st[b, rows, :] + rest * vals[j][hh][:, s : s + 1]
                        st[b, rows, :] = new
                        terms[j][hh].append(quer * new)
            for j in range(2):
                for hh in range(2):
                    term = jnp.concatenate(terms[j][hh], axis=0)
                    high = term.astype(BF16)
                    low = (term - high.astype(F32)).astype(BF16)
                    sums = jnp.dot(high, ones, preferred_element_type=F32) + jnp.dot(low, ones, preferred_element_type=F32)
                    for s in range(16):
                        read[j][hh] = jnp.where(lane == s0 + s, sums[8 * s : 8 * s + 8], read[j][hh])
        vt[...] = jnp.zeros((128, 128), F32)
        for j in range(2):
            for hh in range(2):
                vt[pl.ds(16 * hh + j, 8, stride=2), :] = read[j][hh]
        rt = jnp.transpose(vt[...])
        tile = rt[0:8]
        for a in range(1, 4):
            tile = tile + pltpu.roll(rt[8 * a : 8 * a + 8], 32 * a, 1)
        gr[b, y * NZ + z] = tile.astype(BF16)
        to_all(gr.at[b], base + 3)
        if b == 0:
            arrived(wo.at[0, pl.ds(0, 12)], so_s.at[2], so_r.at[2])
            send(wo.at[core], wo.at[core], so_s.at[3], so_r.at[3], mate)
            arrived(wide.at[pl.ds(0, 3)], sw.at[1], rw.at[1])
            for p in xp:
                send(wide, wq1.at[x, core], sw.at[2], rw.at[2], p)
                send(own.at[1, pl.ds(64, 64)], wv1.at[x, core], sw.at[3], rw.at[3], p)
            wq1[x, core] = wide[...]
        else:
            z_wait(gg.at[1], 6)
            y_send(gg.at[1], 6)
        y_wait(gg.at[b], base + 2)
        gate = turn([gg[b, i, :, 0].astype(F32) for i in range(NY)])
        all_here(gr.at[b], base + 3)
        read = turn([gr[b, NZ * i : NZ * i + NZ].astype(F32) for i in range(NY)])
        for a in range(4):
            sq = jnp.sum(read[a] * read[a], axis=0)
            for shift in (64, 32):
                sq = sq + pltpu.roll(sq, shift, 1)
            sq = sq + jnp.where(lane % 2 == 0, pltpu.roll(sq, 127, 1), pltpu.roll(sq, 1, 1))
            scale = lax.rsqrt(sq / 128.0 + EPS)
            for k in range(NZ):
                xs[8 * a : 8 * a + 8, 128 * k : 128 * k + 128] = (read[a][k] * scale * gate[a][k]).astype(BF16)
        if b == 0:
            arrived(wo.at[0], so_s.at[3], so_r.at[3])
        branch = jnp.dot(xs[...], wo[b].reshape(2048, 128), preferred_element_type=F32)
        if b == 0:
            fresh = (xres[z] + branch).astype(BF16).astype(F32)
            xres[0] = fresh
            for a in range(4):
                x1b[a] = fresh[8 * a : 8 * a + 8].astype(BF16)
            x1[y * NZ + z] = x1b[y]
            to_all(x1, 4)
            arrived(wq1.at[pl.ds(0, 3), 0], sw.at[2], rw.at[2])
            arrived(wv1.at[pl.ds(0, 3), 0], sw.at[3], rw.at[3])
            send(wq1.at[:, core], wq1.at[:, core], sw.at[4], rw.at[4], mate)
            send(wv1.at[:, core], wv1.at[:, core], sw.at[5], rw.at[5], mate)
            all_here(x1, 4)
        else:
            fresh = xres[0] + branch
            mine = fresh
            for k in range(1, NY):
                mine = jnp.where(y == k, pltpu.roll(fresh, 128 - 32 * k, 1), mine)
            xo_ref[...] = mine[:, :32].astype(BF16)

    for b in range(2):
        all_left(gg.at[b], 4 * b + 2)
        left(gr.at[b, pl.ds(0, NY * NZ - 1)], sx.at[4 * b + 3, 0], rx.at[4 * b + 3, 0])
    left(gq.at[0, pl.ds(0, 7)], sx.at[1, 0], rx.at[1, 0])
    left(gq.at[0, pl.ds(0, 8)], sx.at[1, 2], rx.at[1, 2])
    left(gq.at[pl.ds(0, NY - 1)], sx.at[1, 1], rx.at[1, 1])
    left(gq1.at[pl.ds(0, 60)], sx.at[5, 0], rx.at[5, 0])
    left(x0.at[0, pl.ds(0, 8)], sx.at[0, 0], rx.at[0, 0])
    left(gr.at[0, pl.ds(0, 55)], sx.at[0, 1], rx.at[0, 1])
    left(x1.at[pl.ds(0, NY * NZ - 1)], sx.at[4, 0], rx.at[4, 0])
    left(wt.at[pl.ds(0, NDP - 1)], sw.at[0], rw.at[0])
    left(wide.at[pl.ds(0, 3)], sw.at[1], rw.at[1])
    left(wq1.at[pl.ds(0, 3), 0], sw.at[2], rw.at[2])
    left(wv1.at[pl.ds(0, 3), 0], sw.at[3], rw.at[3])
    left(wq1.at[:, 0], sw.at[4], rw.at[4])
    left(wv1.at[:, 0], sw.at[5], rw.at[5])
    left(gr.at[0, pl.ds(0, NZ - 1)], so_s.at[0], so_r.at[0])
    left(gr.at[0, pl.ds(0, 48)], so_s.at[1], so_r.at[1])
    left(wo.at[0, pl.ds(0, 12)], so_s.at[2], so_r.at[2])
    left(wo.at[0], so_s.at[3], so_r.at[3])


def shards(
    resid, norm_gain, w_query, w_forget, w_value, w_gate, gate_floor, states, out_gain, w_out
):
    st = states.reshape(2, resid.shape[0] * 32, 128)
    vmem = pl.BlockSpec(memory_space=pltpu.VMEM)
    hbm = pl.BlockSpec(memory_space=pl.ANY)
    dma = pltpu.SemaphoreType.DMA
    new_resid, new_states = pl.pallas_call(
        kernel,
        out_shape=(pltpu.VMEM((32, 32), BF16), pltpu.VMEM(st.shape, F32)),
        in_specs=[hbm] * 10,
        out_specs=(vmem, vmem),
        scratch_shapes=[
            pltpu.VMEM((NY, NZ, 8, 128), BF16),
            pltpu.VMEM((NY * NZ, 8, 128), BF16),
            pltpu.VMEM((NY, NZ, 2, 8, 128), BF16),
            pltpu.VMEM((NY * NZ, 2, 8, 128), BF16),
            pltpu.VMEM((2, NY, NZ, 1, 8, 128), BF16),
            pltpu.VMEM((2, NY * NZ, 8, 128), BF16),
            pltpu.VMEM((NDP, 128, 256), BF16),
            pltpu.VMEM((4, 64, 256), BF16),
            pltpu.VMEM((4, 2, 4, 64, 256), BF16),
            pltpu.VMEM((4, 2, 64, 256), BF16),
            pltpu.VMEM((2, NZ, NY, 4, 8, 128), BF16),
            pltpu.VMEM((NZ, 4, 8, 128), BF16),
            pltpu.VMEM((2, 128, 256), BF16),
            pltpu.VMEM((2, 32 * PITCH, 128), F32),
            pltpu.VMEM((32, 2048), BF16),
            pltpu.VMEM((NZ, 32, 128), F32),
            pltpu.VMEM((4, 8, 128), BF16),
            pltpu.VMEM((128, 128), F32),
            pltpu.VMEM((32, 32), BF16),
            pltpu.VMEM((2, 2048), F32),
            pltpu.VMEM((2, 16, 2, 256), BF16),
            pltpu.VMEM((2, 16, 2, 256), BF16),
            pltpu.VMEM((2, 2048), F32),
            pltpu.VMEM((2, 2, 16), F32),
            pltpu.VMEM((16, 2, 2048), BF16),
            dma((8, 3)),
            dma((8, 3)),
            dma((6,)),
            dma((6,)),
            dma((4,)),
            dma((4,)),
            dma((11,)),
        ],
        compiler_params=pltpu.CompilerParams(collective_id=0, has_side_effects=True),
        name="blocks",
    )(
        resid,
        norm_gain,
        w_query.transpose(0, 2, 1),
        w_forget.transpose(0, 2, 1),
        w_value.transpose(0, 2, 3, 1),
        w_gate.transpose(0, 2, 3, 1),
        gate_floor,
        out_gain.transpose(0, 2, 1),
        w_out,
        st,
    )
    return new_resid, new_states.reshape(states.shape)


def solution(mesh):
    return jax.shard_map(
        shards,
        mesh=mesh,
        in_specs=(
            P("dp", "tp"),
            P(),
            P(None, "dp", "tp"),
            P(None, "dp", "tp"),
            P(None, "dp", None, "tp"),
            P(None, "dp", None, "tp"),
            P(),
            P(None, "dp", None, "tp", None),
            P(None, None, "tp"),
            P(None, None, "tp", None),
        ),
        out_specs=(P("dp", "tp"), P(None, "dp", None, "tp", None)),
        check_vma=False,
    )
```

```python
import functools

import jax
import jax.numpy as jnp
from jax import lax
from jax.experimental import pallas as pl
from jax.experimental.pallas import tpu as pltpu
from jax.sharding import PartitionSpec as P

MESH = pl.DeviceIdType.MESH
EPS = 1e-06
F32, BF16 = jnp.float32, jnp.bfloat16
NZ, NY, NDP = 16, 4, 8
PITCH = 24


def lanes():
    return lax.broadcasted_iota(jnp.int32, (8, 128), 1)


def turn(parts):
    group = lax.broadcasted_iota(jnp.int32, parts[0].shape, parts[0].ndim - 1) // 32
    axis = parts[0].ndim - 1
    out = []
    for g in range(4):
        acc = parts[g]
        for p in range(4):
            if p != g:
                acc = jnp.where(group == p, pltpu.roll(parts[p], (32 * (p - g)) % 128, axis), acc)
        out.append(acc)
    return out


def kernel(
    x_hbm, gain_hbm, wq_hbm, wf_hbm, wv_hbm, wg_hbm, floor_hbm, og_hbm, wo_hbm, st_hbm,
    xo_ref, st,
    x0, x1, gq, gq1, gg, gr, wt, wide, wq1, wv1, wo, wsrc, own, kq, xs, xres, x1b, vt,
    x_ref, gain_ref, wv_ref, wg_ref, floor_ref, og_ref, wo_ref,
    sx, rx, sw, rw, so_s, so_r, lsem,
):
    tp = lax.axis_index("tp")
    dp = lax.axis_index("dp")
    z, y = tp // NY, tp % NY
    core = dp % 2
    zdist = (8, 7, 9, 6, 10, 5, 11, 4, 12, 3, 13, 2, 14, 1, 15)
    zclose = (4, -4, 3, -3, 2, -2, 1, -1)
    zi = [lax.rem(z + k, NZ) for k in zdist]
    zp = [{"tp": i * NY + y} for i in zi]
    yp = [{"tp": z * NY + lax.rem(y + k, NY)} for k in (2, 1, 3)]
    dpp = [{"dp": lax.rem(dp + k, NDP)} for k in (4, 3, 5, 2, 6, 1, 7)]
    mate = {"dp": dp + 1 - 2 * core}
    x = dp // 2
    xp = [{"dp": lax.rem(x + k, 4) * 2 + core} for k in (2, 1, 3)]
    cls, turnover = z % 4, z // 4

    bar = pltpu.get_barrier_semaphore()
    zc = [{"tp": lax.rem(z + NZ + k, NZ) * NY + y} for k in zclose]
    for p in zc + yp + dpp:
        pl.semaphore_signal(bar, inc=1, device_id=p, device_id_type=MESH)
    def load(src, dst, i):
        copy = pltpu.make_async_copy(src, dst, lsem.at[i])
        copy.start()
        return copy

    x_load = load(x_hbm, x_ref, 0)
    weight_loads = [
        load(wq_hbm, own.at[:, pl.ds(0, 32)], 1),
        load(wf_hbm, own.at[:, pl.ds(32, 32)], 2),
        load(wv_hbm, wv_ref, 3),
        load(wg_hbm, wg_ref, 4),
    ]
    small_loads = [
        load(wo_hbm.at[core], wo_ref, 5),
        load(gain_hbm, gain_ref, 6),
        load(floor_hbm, floor_ref, 7),
        load(og_hbm, og_ref, 8),
    ]
    loads = [load(st_hbm.at[b], st.at[b], 9 + b) for b in range(2)]
    x_load.wait()
    x_in = x_ref[...].astype(F32)
    x0[y, 8] = jnp.concatenate([x_in[8 * a : 8 * a + 8] for a in range(4)], axis=1).astype(BF16)
    pl.semaphore_wait(bar, len(zc) + len(yp) + len(dpp))

    def send(src, dst, s, r, p):
        pltpu.make_async_remote_copy(src, dst, s, r, device_id=p, device_id_type=MESH).start()

    def arrived(ref, s, r):
        pltpu.make_async_remote_copy(ref, ref, s, r, device_id=mate, device_id_type=MESH).wait_recv()

    def left(ref, s, r):
        pltpu.make_async_remote_copy(ref, ref, s, r, device_id=mate, device_id_type=MESH).wait_send()

    def z_send(buf, i):
        for p in zp:
            send(buf.at[y, z], buf.at[y, z], sx.at[i, 0], rx.at[i, 0], p)

    def z_wait(buf, i):
        arrived(buf.at[0, pl.ds(0, NZ - 1)], sx.at[i, 0], rx.at[i, 0])

    def y_send(buf, i):
        for p in yp:
            send(buf.at[y], buf.at[y], sx.at[i, 1], rx.at[i, 1], p)

    def y_wait(buf, i):
        arrived(buf.at[pl.ds(0, NY - 1)], sx.at[i, 1], rx.at[i, 1])

    def to_all(buf, i):
        tile = buf.at[y * NZ + z]
        for j in zi:
            for k in (2, 1, 3, 0):
                send(tile, tile, sx.at[i, 0], rx.at[i, 0], {"tp": j * NY + lax.rem(y + k, NY)})
        for p in yp:
            send(tile, tile, sx.at[i, 0], rx.at[i, 0], p)

    def all_here(buf, i):
        arrived(buf.at[pl.ds(0, NY * NZ - 1)], sx.at[i, 0], rx.at[i, 0])

    def all_left(buf, i):
        left(buf.at[0, pl.ds(0, NZ - 1)], sx.at[i, 0], rx.at[i, 0])
        left(buf.at[pl.ds(0, NY - 1)], sx.at[i, 1], rx.at[i, 1])

    for k, p in zip(zclose, zc):
        send(x0.at[y, 8], x0.at[y, 8 - k], sx.at[0, 0], rx.at[0, 0], p)
    for copy in weight_loads:
        copy.wait()
    for b in range(2):
        own[b, 64:96, :] = wv_ref[b].reshape(32, 256)
        own[b, 96:128, :] = wg_ref[b].reshape(32, 256)
        if b == 0:
            wt[dp] = own[0]
            for p in dpp:
                send(own.at[0], wt.at[dp], sw.at[0], rw.at[0], p)
    for copy in small_loads:
        copy.wait()
    wide[turnover] = own[1, 0:64, :]
    wv1[x, core] = own[1, 64:128, :]
    for k in range(NZ):
        wsrc[k] = wo_ref[:, :, 128 * k : 128 * k + 128].reshape(4, 8, 128)
    wo[core, z, y, x] = wsrc[z, x]
    spot = lax.broadcasted_iota(jnp.int32, (16, 128), 1) % 32
    head = lax.broadcasted_iota(jnp.int32, (16, 128), 0)
    gains = []
    for b in range(2):
        row = jnp.zeros((1, 128), F32)
        for j in range(2):
            pick = jnp.where(spot == 2 * head + j, 1.0, 0.0)
            row = row + jnp.dot(og_ref[b, j : j + 1, :], pick, precision=lax.Precision.HIGHEST, preferred_element_type=F32)
        gains.append(row)
    arrived(x0.at[0, pl.ds(0, 8)], sx.at[0, 0], rx.at[0, 0])
    for k in (2, 1, 3, 0):
        yk = lax.rem(y + k, NY)
        up = {"tp": lax.rem(z + 4, NZ) * NY + yk}
        down = {"tp": lax.rem(z + NZ - 4, NZ) * NY + yk}
        send(x0.at[y, pl.ds(4, 4)], x0.at[y, pl.ds(0, 4)], sx.at[0, 1], rx.at[0, 1], up)
        send(x0.at[y, pl.ds(9, 3)], x0.at[y, pl.ds(13, 3)], sx.at[0, 1], rx.at[0, 1], down)
    for p in yp:
        send(x0.at[y, pl.ds(4, 9)], x0.at[y, pl.ds(4, 9)], sx.at[0, 1], rx.at[0, 1], p)
    for i, p in zip(zi, zp):
        send(wsrc.at[i, x], wo.at[core, z, y, x], so_s.at[0], so_r.at[0], p)
    arrived(wt.at[pl.ds(0, NDP - 1)], sw.at[0], rw.at[0])
    arrived(gr.at[0, pl.ds(0, 55)], sx.at[0, 1], rx.at[0, 1])

    def project(weights, width, inv):
        total = jnp.zeros((32, width), F32)
        for d in range(NDP):
            part = lax.dot_general(
                xs[:, 256 * d : 256 * d + 256], weights(d), (((1,), (1,)), ((), ())), preferred_element_type=F32
            )
            total = total + part.astype(BF16).astype(F32)
        return (total * inv).astype(BF16).astype(F32)

    for b in range(2):
        base = 4 * b
        if b == 0:
            tiles = [[], [], [], []]
            for k in range(NZ):
                slot = lax.rem(k + 24 - z, NZ)
                four = turn([x0[i, slot].astype(F32) for i in range(NY)])
                for a in range(4):
                    tiles[a].append(four[a])
                    xres[k, 8 * a : 8 * a + 8, :] = four[a]
            tiles = [jnp.stack(t) for t in tiles]
        else:
            tiles = [x1[NZ * a : NZ * a + NZ].astype(F32) for a in range(NY)]
        inv = []
        for a in range(4):
            sq = jnp.sum(jnp.sum(tiles[a] * tiles[a], axis=0), axis=1, keepdims=True)
            inv.append(lax.rsqrt(sq / (NZ * 128) + EPS))
            for k in range(NZ):
                scaled = tiles[a][k] * gain_ref[b : b + 1, 128 * k : 128 * k + 128]
                xs[8 * a : 8 * a + 8, 128 * k : 128 * k + 128] = scaled.astype(BF16)
        inv = jnp.concatenate(inv, axis=0)
        if b == 0:
            proj = project(lambda d: wt[d], 128, inv)
            packed = turn([proj[8 * a : 8 * a + 8] for a in range(4)])
            gq[y, 8, 0] = packed[0].astype(BF16)
            gq[y, 8, 1] = packed[1].astype(BF16)
            for k in (8, 7, -7, 6, -6, 5, -5, 4, -4, 3, -3, 2, -2, 1, -1):
                to = {"tp": lax.rem(z + NZ + k, NZ) * NY + y}
                side = 0 if abs(k) > 5 else 2
                send(gq.at[y, 8], gq.at[y, 8 - k], sx.at[1, side], rx.at[1, side], to)
            gate = packed[3]
        else:
            arrived(wq1.at[:, 0], sw.at[4], rw.at[4])
            arrived(wv1.at[:, 0], sw.at[5], rw.at[5])
            proj = project(lambda d: wq1[d // 2, d % 2].reshape(256, 256), 256, inv)
            unit = (y * 4 + cls) * 4
            for half in range(2):
                packed = turn([proj[8 * a : 8 * a + 8, 128 * half : 128 * half + 128] for a in range(4)])
                for q in range(2):
                    gq1[unit + 2 * half + q, 0] = packed[2 * q].astype(BF16)
                    gq1[unit + 2 * half + q, 1] = packed[2 * q + 1].astype(BF16)
            for k, first, count in ((2, 2, 2), (-2, 0, 2), (1, 0, 4), (-1, 0, 4), (0, 0, 4)):
                for j in (2, 1, 3) if k == 0 else (2, 1, 3, 0):
                    to = {"tp": lax.rem(z + NZ + k, NZ) * NY + lax.rem(y + j, NY)}
                    part = gq1.at[pl.ds(unit + first, count)]
                    send(part, part, sx.at[5, 0], rx.at[5, 0], to)
            proj = jnp.concatenate([project(lambda d: wv1[d // 2, d % 2], 64, inv), jnp.zeros((32, 64), F32)], axis=1)
            gate = turn([proj[8 * a : 8 * a + 8] for a in range(4)])[1]
        gg[b, y, z, 0] = (gains[b] * (gate / (1.0 + jnp.exp(-gate)))).astype(BF16)
        if b == 1:
            z_send(gg.at[b], base + 2)
        else:
            arrived(gr.at[0, pl.ds(0, NZ - 1)], so_s.at[0], so_r.at[0])
            for p in yp:
                send(wo.at[core, :, y, x], wo.at[core, :, y, x], so_s.at[1], so_r.at[1], p)
        vt[...] = jnp.transpose(jnp.concatenate([proj, jnp.zeros((96, 128), F32)], axis=0))
        if b == 0:
            arrived(gq.at[0, pl.ds(0, 10)], sx.at[1, 2], rx.at[1, 2])
            for p in yp:
                send(gq.at[y, pl.ds(3, 11)], gq.at[y, pl.ds(3, 11)], sx.at[1, 1], rx.at[1, 1], p)
            z_send(gg.at[0], 2)
            arrived(gq.at[0, pl.ds(0, 5)], sx.at[1, 0], rx.at[1, 0])
            for p in yp:
                send(gq.at[y, pl.ds(0, 3)], gq.at[y, pl.ds(0, 3)], sx.at[1, 1], rx.at[1, 1], p)
                send(gq.at[y, pl.ds(14, 2)], gq.at[y, pl.ds(14, 2)], sx.at[1, 1], rx.at[1, 1], p)
            for k in (8, 4, 12):
                to = {"tp": lax.rem(z + k, NZ) * NY + y}
                send(own.at[1, pl.ds(0, 64)], wide.at[turnover], sw.at[1], rw.at[1], to)
            arrived(gr.at[0, pl.ds(0, 48)], so_s.at[1], so_r.at[1])
            for p in xp:
                send(wo.at[core, :, :, x], wo.at[core, :, :, x], so_s.at[2], so_r.at[2], p)
            y_wait(gq, 1)
        else:
            arrived(gq1.at[pl.ds(0, 60)], sx.at[5, 0], rx.at[5, 0])
        for k in range(NZ):
            low = floor_ref[b : b + 1, 128 * k : 128 * k + 128]
            for p in range(2):
                if b == 0:
                    four = turn([gq[i, lax.rem(k + 24 - z, NZ), p].astype(F32) for i in range(NY)])
                else:
                    four = turn([gq1[(4 * i + k % 4) * 4 + k // 4, p].astype(F32) for i in range(NY)])
                for a in range(4):
                    rows = pl.ds(8 * a * PITCH + k, 8, stride=PITCH)
                    if p == 0:
                        kq[1, rows, :] = four[a]
                    else:
                        kq[0, rows, :] = low + (1.0 - low) * (1.0 / (1.0 + jnp.exp(-four[a])))
        loads[b].wait()
        if b == 0:
            z_wait(gg.at[0], 2)
            y_send(gg.at[0], 2)
        lane = lanes()
        ones = jnp.ones((128, 128), BF16)
        read = [[jnp.zeros((8, 128), F32) for _ in range(2)] for _ in range(2)]
        first = 64 if b == 0 else 0
        vals = [[vt[pl.ds(first + 16 * hh + j, 8, stride=2), :] for hh in range(2)] for j in range(2)]
        for s0 in range(0, 32, 16):
            terms = [[[], []], [[], []]]
            for s in range(s0, s0 + 16):
                for hh in range(2):
                    keep = kq[0, s * PITCH + 8 * hh : s * PITCH + 8 * hh + 8, :]
                    quer = kq[1, s * PITCH + 8 * hh : s * PITCH + 8 * hh + 8, :]
                    rest = 1.0 - keep
                    for j in range(2):
                        rows = pl.ds(s * 32 + hh * 16 + j, 8, stride=2)
                        new = keep * st[b, rows, :] + rest * vals[j][hh][:, s : s + 1]
                        st[b, rows, :] = new
                        terms[j][hh].append(quer * new)
            for j in range(2):
                for hh in range(2):
                    term = jnp.concatenate(terms[j][hh], axis=0)
                    high = term.astype(BF16)
                    low = (term - high.astype(F32)).astype(BF16)
                    sums = jnp.dot(high, ones, preferred_element_type=F32) + jnp.dot(low, ones, preferred_element_type=F32)
                    for s in range(16):
                        read[j][hh] = jnp.where(lane == s0 + s, sums[8 * s : 8 * s + 8], read[j][hh])
        vt[...] = jnp.zeros((128, 128), F32)
        for j in range(2):
            for hh in range(2):
                vt[pl.ds(16 * hh + j, 8, stride=2), :] = read[j][hh]
        rt = jnp.transpose(vt[...])
        tile = rt[0:8]
        for a in range(1, 4):
            tile = tile + pltpu.roll(rt[8 * a : 8 * a + 8], 32 * a, 1)
        gr[b, y * NZ + z] = tile.astype(BF16)
        to_all(gr.at[b], base + 3)
        if b == 0:
            arrived(wo.at[0, pl.ds(0, 12)], so_s.at[2], so_r.at[2])
            send(wo.at[core], wo.at[core], so_s.at[3], so_r.at[3], mate)
            arrived(wide.at[pl.ds(0, 3)], sw.at[1], rw.at[1])
            for p in xp:
                send(wide, wq1.at[x, core], sw.at[2], rw.at[2], p)
                send(own.at[1, pl.ds(64, 64)], wv1.at[x, core], sw.at[3], rw.at[3], p)
            wq1[x, core] = wide[...]
        else:
            z_wait(gg.at[1], 6)
            y_send(gg.at[1], 6)
        y_wait(gg.at[b], base + 2)
        gate = turn([gg[b, i, :, 0].astype(F32) for i in range(NY)])
        all_here(gr.at[b], base + 3)
        read = turn([gr[b, NZ * i : NZ * i + NZ].astype(F32) for i in range(NY)])
        for a in range(4):
            sq = jnp.sum(read[a] * read[a], axis=0)
            for shift in (64, 32):
                sq = sq + pltpu.roll(sq, shift, 1)
            sq = sq + jnp.where(lane % 2 == 0, pltpu.roll(sq, 127, 1), pltpu.roll(sq, 1, 1))
            scale = lax.rsqrt(sq / 128.0 + EPS)
            for k in range(NZ):
                xs[8 * a : 8 * a + 8, 128 * k : 128 * k + 128] = (read[a][k] * scale * gate[a][k]).astype(BF16)
        if b == 0:
            arrived(wo.at[0], so_s.at[3], so_r.at[3])
        branch = jnp.dot(xs[...], wo[b].reshape(2048, 128), preferred_element_type=F32)
        if b == 0:
            fresh = (xres[z] + branch).astype(BF16).astype(F32)
            xres[0] = fresh
            for a in range(4):
                x1b[a] = fresh[8 * a : 8 * a + 8].astype(BF16)
            x1[y * NZ + z] = x1b[y]
            to_all(x1, 4)
            arrived(wq1.at[pl.ds(0, 3), 0], sw.at[2], rw.at[2])
            arrived(wv1.at[pl.ds(0, 3), 0], sw.at[3], rw.at[3])
            send(wq1.at[:, core], wq1.at[:, core], sw.at[4], rw.at[4], mate)
            send(wv1.at[:, core], wv1.at[:, core], sw.at[5], rw.at[5], mate)
            all_here(x1, 4)
        else:
            fresh = xres[0] + branch
            mine = fresh
            for k in range(1, NY):
                mine = jnp.where(y == k, pltpu.roll(fresh, 128 - 32 * k, 1), mine)
            xo_ref[...] = mine[:, :32].astype(BF16)

    for b in range(2):
        all_left(gg.at[b], 4 * b + 2)
        left(gr.at[b, pl.ds(0, NY * NZ - 1)], sx.at[4 * b + 3, 0], rx.at[4 * b + 3, 0])
    left(gq.at[0, pl.ds(0, 5)], sx.at[1, 0], rx.at[1, 0])
    left(gq.at[0, pl.ds(0, 10)], sx.at[1, 2], rx.at[1, 2])
    left(gq.at[pl.ds(0, NY - 1)], sx.at[1, 1], rx.at[1, 1])
    left(gq1.at[pl.ds(0, 60)], sx.at[5, 0], rx.at[5, 0])
    left(x0.at[0, pl.ds(0, 8)], sx.at[0, 0], rx.at[0, 0])
    left(gr.at[0, pl.ds(0, 55)], sx.at[0, 1], rx.at[0, 1])
    left(x1.at[pl.ds(0, NY * NZ - 1)], sx.at[4, 0], rx.at[4, 0])
    left(wt.at[pl.ds(0, NDP - 1)], sw.at[0], rw.at[0])
    left(wide.at[pl.ds(0, 3)], sw.at[1], rw.at[1])
    left(wq1.at[pl.ds(0, 3), 0], sw.at[2], rw.at[2])
    left(wv1.at[pl.ds(0, 3), 0], sw.at[3], rw.at[3])
    left(wq1.at[:, 0], sw.at[4], rw.at[4])
    left(wv1.at[:, 0], sw.at[5], rw.at[5])
    left(gr.at[0, pl.ds(0, NZ - 1)], so_s.at[0], so_r.at[0])
    left(gr.at[0, pl.ds(0, 48)], so_s.at[1], so_r.at[1])
    left(wo.at[0, pl.ds(0, 12)], so_s.at[2], so_r.at[2])
    left(wo.at[0], so_s.at[3], so_r.at[3])


def shards(
    resid, norm_gain, w_query, w_forget, w_value, w_gate, gate_floor, states, out_gain, w_out
):
    st = states.reshape(2, resid.shape[0] * 32, 128)
    vmem = pl.BlockSpec(memory_space=pltpu.VMEM)
    hbm = pl.BlockSpec(memory_space=pl.ANY)
    dma = pltpu.SemaphoreType.DMA
    new_resid, new_states = pl.pallas_call(
        kernel,
        out_shape=(pltpu.VMEM((32, 32), BF16), pltpu.VMEM(st.shape, F32)),
        in_specs=[hbm] * 10,
        out_specs=(vmem, vmem),
        scratch_shapes=[
            pltpu.VMEM((NY, NZ, 8, 128), BF16),
            pltpu.VMEM((NY * NZ, 8, 128), BF16),
            pltpu.VMEM((NY, NZ, 2, 8, 128), BF16),
            pltpu.VMEM((NY * NZ, 2, 8, 128), BF16),
            pltpu.VMEM((2, NY, NZ, 1, 8, 128), BF16),
            pltpu.VMEM((2, NY * NZ, 8, 128), BF16),
            pltpu.VMEM((NDP, 128, 256), BF16),
            pltpu.VMEM((4, 64, 256), BF16),
            pltpu.VMEM((4, 2, 4, 64, 256), BF16),
            pltpu.VMEM((4, 2, 64, 256), BF16),
            pltpu.VMEM((2, NZ, NY, 4, 8, 128), BF16),
            pltpu.VMEM((NZ, 4, 8, 128), BF16),
            pltpu.VMEM((2, 128, 256), BF16),
            pltpu.VMEM((2, 32 * PITCH, 128), F32),
            pltpu.VMEM((32, 2048), BF16),
            pltpu.VMEM((NZ, 32, 128), F32),
            pltpu.VMEM((4, 8, 128), BF16),
            pltpu.VMEM((128, 128), F32),
            pltpu.VMEM((32, 32), BF16),
            pltpu.VMEM((2, 2048), F32),
            pltpu.VMEM((2, 16, 2, 256), BF16),
            pltpu.VMEM((2, 16, 2, 256), BF16),
            pltpu.VMEM((2, 2048), F32),
            pltpu.VMEM((2, 2, 16), F32),
            pltpu.VMEM((16, 2, 2048), BF16),
            dma((8, 3)),
            dma((8, 3)),
            dma((6,)),
            dma((6,)),
            dma((4,)),
            dma((4,)),
            dma((11,)),
        ],
        compiler_params=pltpu.CompilerParams(collective_id=0, has_side_effects=True),
        name="blocks",
    )(
        resid,
        norm_gain,
        w_query.transpose(0, 2, 1),
        w_forget.transpose(0, 2, 1),
        w_value.transpose(0, 2, 3, 1),
        w_gate.transpose(0, 2, 3, 1),
        gate_floor,
        out_gain.transpose(0, 2, 1),
        w_out,
        st,
    )
    return new_resid, new_states.reshape(states.shape)


def solution(mesh):
    return jax.shard_map(
        shards,
        mesh=mesh,
        in_specs=(
            P("dp", "tp"),
            P(),
            P(None, "dp", "tp"),
            P(None, "dp", "tp"),
            P(None, "dp", None, "tp"),
            P(None, "dp", None, "tp"),
            P(),
            P(None, "dp", None, "tp", None),
            P(None, None, "tp"),
            P(None, None, "tp", None),
        ),
        out_specs=(P("dp", "tp"), P(None, "dp", None, "tp", None)),
        check_vma=False,
    )
```
